32 devices in a mesh: sp: 8 (over z, x), tp: 4 (over y, core).
Axes of the slice: x: 2, y: 2, z: 4, core: 2. Of those that a mesh axis runs over, the one named last changes fastest.
Arguments:
- residual_in: bfloat16 [2048, 2048], P(('sp', 'tp')), may hold values from -6 to 6
- queries: bfloat16 [2048, 512], P('sp', 'tp'), may hold values from -6 to 6
- key_rows: bfloat16 [2048, 512], P('sp', 'tp'), may hold values from -6 to 6
- value_rows: bfloat16 [2048, 1024], P('sp', 'tp'), may hold values from -6 to 6
- out_gate: bfloat16 [2048, 1024], P('sp', 'tp'), may hold values from -6 to 6
- decay_logit: float32 [2048, 512], P('sp', 'tp'), may hold values from -30 to 30
- head_gain: bfloat16 [128], replicated, may hold values from 0.099609375 to 1.8984375
- w_out: bfloat16 [1024, 2048], replicated, may hold values from -0.1875 to 0.1875
- ffn_gain: bfloat16 [2048], replicated, may hold values from 0.099609375 to 1.8984375
- routing: int32 [2048, 4], P('sp'), may hold values from 0 to 7, all different within a row; in each aligned block of 64 rows (0 to 63, 64 to 127, ...) at most 64 rows name the same one
- route_weight: float32 [2048, 4], P(('sp', 'tp')), may hold values from 0.05 to 0.6
- w_gate: bfloat16 [8, 2048, 2048], P('sp', None, 'tp'), may hold values from -4 to 4
- w_up: bfloat16 [8, 2048, 2048], P('sp', None, 'tp'), may hold values from -4 to 4
- w_down: bfloat16 [8, 2048, 2048], P('sp', 'tp'), may hold values from -0.125 to 0.125
Outputs:
- layer_out: bfloat16 [2048, 2048], P(('sp', 'tp'))
The draws below stay inside these ranges and needn't reach their ends.
Inputs may be any that keep to these rules, and one draw needn't show every extreme that they name: `routing`: each row names 4 different experts. In each aligned block of 64 rows no expert is named more than 64 times, a bound that some blocks reach.
All inputs are finite; a program needn't handle non-finite values.
Results may differ from the reference program's by a relative error of at most 0.03.
Values may be sent and summed in bfloat16 or wider, within the bound.
A program may use at most 128 MiB of HBM per device.

```python
import math
import jax
import jax.numpy as jnp
import numpy as np
from jax import lax

D = 2048
HEADS = 8
DK = 64
DV = 128
FF = 2048
TOP = 4
BLOCK = 64
TOK_DEV = 256
TOKEN_COUNT = 2048
EXPERTS = 8
QROWS = 64
CAP = 64
N_TP = 4


def draw_decay_logit(key, part):
    random_subkeys = jax.random.split(jax.random.fold_in(key, 31), 7)
    channels = HEADS * DK
    share_fast = 0.5
    fast_head = jax.random.uniform(random_subkeys[0], (HEADS,)) < share_fast
    fast_channel = jnp.repeat(fast_head, DK)
    fast_rate = jnp.exp(jax.random.uniform(random_subkeys[1], (channels,), minval=jnp.log(1.0 / 50.0), maxval=jnp.log(1.0 / 15.0)))
    slow_rate = jnp.exp(jax.random.uniform(random_subkeys[2], (channels,), minval=jnp.log(0.3), maxval=0.0)) * 0.7 / TOKEN_COUNT
    base_rate = jnp.where(fast_channel, fast_rate, slow_rate)
    span_count = TOKEN_COUNT // TOK_DEV
    span_factor = jnp.repeat(jnp.exp(jax.random.uniform(random_subkeys[3], (span_count,), minval=jnp.log(0.5), maxval=jnp.log(2.0))), TOK_DEV)
    jitter = jnp.exp(0.6 * jax.random.truncated_normal(random_subkeys[4], -3.0, 3.0, (TOKEN_COUNT, channels)))
    stepwise_results = base_rate[None, :] * span_factor[:, None] * jitter
    spike_location = jax.random.randint(random_subkeys[5], (3,), 0, TOKEN_COUNT)
    spike_penalty = jax.random.uniform(random_subkeys[6], (3,), minval=0.2, maxval=0.45)
    position_indices = jnp.arange(TOKEN_COUNT)
    spike_increment = jnp.sum(jnp.where(position_indices[:, None] == spike_location[None, :], -jnp.log(1.0 - spike_penalty)[None, :], 0.0), axis=1)
    stepwise_results = stepwise_results + spike_increment[:, None]
    scaled = 16.0 * stepwise_results
    return -jnp.log(jnp.expm1(scaled))


def column_scaled(key, salt_value):
    random_subkeys = jax.random.split(jax.random.fold_in(key, salt_value), 2)
    lowest = 0.3
    highest = 2.5
    scales = jnp.exp(jax.random.uniform(random_subkeys[0], (EXPERTS, 1, FF), minval=jnp.log(lowest), maxval=jnp.log(highest)))
    entries = jax.random.truncated_normal(random_subkeys[1], -4.0, 4.0, (EXPERTS, D, FF))
    return entries * scales * D ** (-0.5)


def draw_w_gate(key, part):
    return column_scaled(key, 11).astype(jnp.bfloat16)


def draw_w_up(key, part):
    return column_scaled(key, 12).astype(jnp.bfloat16)


def block_levels(rng, shape, pieces, least, top_value):
    level = 1.0
    for dim, shards_of in pieces:
        draws = jax.random.uniform(jax.random.fold_in(jax.random.fold_in(rng, 6), dim), (shards_of,), jnp.float32, least / len(pieces), top_value / len(pieces))
        level = level * jnp.repeat(jnp.exp(draws), shape[dim] // shards_of).reshape((-1,) + (1,) * (len(shape) - 1 - dim))
    return level


def deal_out(rng, own, number, rows, number_of, top, limit, skew):
    sequence = jax.random.permutation(rng, number_of)
    crowded, ordinary = shares(number_of, rows * top, limit, skew, True), shares(number_of, rows * top, limit, skew, False)
    places = jnp.arange(number_of)

    def named(tallies, turn):
        used = int((tallies > 0).sum())
        fixed = max(1, used // 4)
        shifted = fixed + (places - fixed + turn * (used - fixed)) % max(1, number_of - fixed)
        return jnp.zeros((number_of,), jnp.int32).at[sequence[jnp.where(places < fixed, places, shifted)]].set(jnp.asarray(tallies, jnp.int32))

    tallies = jnp.where(number % 4 == 0, named(crowded, number // 4), named(ordinary, number - number // 4 - 1))
    mixed = jax.random.permutation(jax.random.fold_in(own, 3), number_of)
    source_of, receiver = mixed[0:number_of // 2 * 2:2], mixed[1:number_of // 2 * 2:2]
    margin = jnp.minimum(tallies[source_of] - 1, limit - tallies[receiver]) // 2
    margin = jnp.where((source_of == sequence[0]) | (receiver == sequence[0]) | (tallies[receiver] == 0), 0, jnp.maximum(margin, 0))
    shifted = jax.random.randint(jax.random.fold_in(own, 4), (number_of // 2,), 0, 1 << 20) % (margin + 1)
    tallies = tallies.at[source_of].add(-shifted).at[receiver].add(shifted)
    items = jnp.searchsorted(jnp.cumsum(tallies), jnp.arange(rows * top), side="right").astype(jnp.int32)
    listing = items.reshape(top, rows).T
    listing = listing[jax.random.permutation(jax.random.fold_in(own, 1), rows)]
    turn = jax.random.randint(jax.random.fold_in(own, 2), (rows, 1), 0, top)
    return jnp.take_along_axis(listing, (jnp.arange(top)[None, :] + turn) % top, axis=1)


def shares(amount, total, reach, skew, full):
    weights = [(1 << 20) // math.isqrt(rank ** skew) + 1 for rank in range(1, amount + 1)]
    largest = reach if full else min(reach, max(-(-total // amount), total * weights[0] // sum(weights)))
    least = 1 if total - largest >= amount - 1 else 0
    counts, surplus = [largest] + [least] * (amount - 1), total - largest - least * (amount - 1)
    while surplus > 0:
        free = [i for i in range(1, amount) if counts[i] < largest] or [i for i in range(1, amount) if counts[i] < reach]
        whole, left = sum([weights[i] for i in free]), surplus
        for i in free:
            more = min(reach - counts[i], max(1, left * weights[i] // whole), surplus)
            counts[i] = counts[i] + more
            surplus = surplus - more
    return np.array(counts)


def normal_values(rng, extent, scale, bound, cuts=(), held_as=jnp.bfloat16):
    values = scale * jax.random.normal(rng, extent, jnp.float32)
    if cuts:
        values = values * block_levels(rng, extent, cuts, -0.22, 0.18)
    return jnp.clip(values, -bound, bound).astype(held_as)


def setup_inputs(seed: int = 0) -> dict:
    arg_keys = jax.random.split(jax.random.key(seed), 15)
    residual_in = normal_values(arg_keys[0], (TOKEN_COUNT, D), 1.0, 6.0, ((0, 32),))
    queries = normal_values(arg_keys[1], (TOKEN_COUNT, HEADS * DK), 1.0, 6.0, ((0, 8), (1, 4)))
    key_rows = normal_values(arg_keys[2], (TOKEN_COUNT, HEADS * DK), 1.0, 6.0, ((0, 8), (1, 4)))
    value_rows = normal_values(arg_keys[3], (TOKEN_COUNT, HEADS * DV), 1.0, 6.0, ((0, 8), (1, 4)))
    out_gate = normal_values(arg_keys[4], (TOKEN_COUNT, HEADS * DV), 1.0, 6.0, ((0, 8), (1, 4)))
    decay_logit = draw_decay_logit(jax.random.fold_in(arg_keys[14], 71), 0)
    head_gain = jnp.clip(1.0 + 0.18 * jax.random.normal(arg_keys[6], (DV,), jnp.float32), 0.099609375, 1.8984375).astype(jnp.bfloat16)
    w_out = normal_values(arg_keys[7], (HEADS * DV, D), (HEADS * DV) ** -0.5, 0.1875)
    ffn_gain = jnp.clip(1.0 + 0.18 * jax.random.normal(arg_keys[8], (D,), jnp.float32), 0.099609375, 1.8984375).astype(jnp.bfloat16)
    routing_keys = jax.random.split(jax.random.fold_in(arg_keys[9], 1), TOKEN_COUNT // QROWS)
    routing_turns = jax.random.permutation(jax.random.fold_in(arg_keys[9], 3), TOKEN_COUNT // QROWS)
    routing = jax.vmap(lambda own, number: deal_out(jax.random.fold_in(arg_keys[9], 2), own, number, QROWS, EXPERTS, TOP, CAP, 2))(routing_keys, routing_turns).reshape((TOKEN_COUNT, TOP))
    route_weight = jnp.clip(jnp.exp(math.log(0.6) - 2.4849067 * jax.random.uniform(arg_keys[10], (TOKEN_COUNT, TOP), jnp.float32) ** block_levels(arg_keys[10], (TOKEN_COUNT, TOP), ((0, 32),), -0.2, 0.2)), 0.05, 0.6)
    w_gate = draw_w_gate(jax.random.fold_in(arg_keys[14], 71), 0)
    w_up = draw_w_up(jax.random.fold_in(arg_keys[14], 71), 0)
    w_down = normal_values(arg_keys[13], (EXPERTS, FF, D), FF ** -0.5, 0.125, ((0, 8), (1, 4)))
    return dict(residual_in=residual_in, queries=queries, key_rows=key_rows, value_rows=value_rows, out_gate=out_gate, decay_logit=decay_logit, head_gain=head_gain, w_out=w_out, ffn_gain=ffn_gain, routing=routing, route_weight=route_weight, w_gate=w_gate, w_up=w_up, w_down=w_down)


DECAY_TEMP = 16.0
CLAMP_LIMIT = 7.0
SIGMOID_SLOPE = 1.702
NORM_EPS = 1e-06
EXACT_PRECISION = lax.Precision.HIGHEST

def block_parts(query_blk, key_blk, value_blk, logdecay_blk):
    cumulative = jnp.cumsum(logdecay_blk, axis=2)
    length = cumulative.shape[2]
    causal = (jnp.arange(length)[:, None] >= jnp.arange(length)[None, :])[:, :, None]
    spread = cumulative[:, :, :, None, :] - cumulative[:, :, None, :, :]
    weighted = query_blk[:, :, :, None, :] * jnp.exp(jnp.where(causal, spread, -jnp.inf))
    scores = jnp.einsum('nhtsk,nhsk->nhts', weighted, key_blk, precision=EXACT_PRECISION)
    inner_part = jnp.einsum('nhts,nhsv->nhtv', scores, value_blk, precision=EXACT_PRECISION)
    ending = cumulative[:, :, -1:, :]
    contrib = jnp.einsum('nhsk,nhsv->nhkv', key_blk * jnp.exp(ending - cumulative), value_blk, precision=EXACT_PRECISION)
    return (inner_part, query_blk * jnp.exp(cumulative), contrib, jnp.exp(ending[:, :, 0, :]))

def carry_blocks(query_dec, contrib, passing, begin):

    def advance(recurrent_state, inputs):
        current_query, contrib_now, passing_now = inputs
        state_readout = jnp.einsum('uaz,uze->uae', current_query, recurrent_state, precision=EXACT_PRECISION)
        return (passing_now[..., None] * recurrent_state + contrib_now, state_readout)
    final_state, readouts = lax.scan(advance, begin, (query_dec, contrib, passing))
    return (readouts, final_state)

def finish_heads(blocks_out, head_gain, out_gate):
    count_blk, head_count, length, head_width = blocks_out.shape
    tokens = count_blk * length
    attended = blocks_out.transpose(0, 2, 1, 3).reshape(tokens, head_count, head_width)
    inv_scale = lax.rsqrt(lax.optimization_barrier(jnp.mean(attended * attended, axis=-1, keepdims=True)) + NORM_EPS)
    headed = attended * inv_scale * head_gain.astype(jnp.float32)
    gated = headed.reshape(tokens, head_count * head_width) * jax.nn.silu(out_gate.astype(jnp.float32))
    return gated.astype(jnp.bfloat16)

def norm_rows(residual, gain_vec):
    values = residual.astype(jnp.float32)
    inv_scale = lax.rsqrt(lax.optimization_barrier(jnp.mean(values * values, axis=-1, keepdims=True)) + NORM_EPS)
    return (values * inv_scale * gain_vec.astype(jnp.float32)).astype(jnp.bfloat16)

def clamped_unit(gate_pre, up_pre):
    gate_cut = jnp.minimum(gate_pre, CLAMP_LIMIT)
    up_cut = jnp.clip(up_pre, -CLAMP_LIMIT, CLAMP_LIMIT)
    return (up_cut + 1.0) * (gate_cut * jax.nn.sigmoid(SIGMOID_SLOPE * gate_cut))

def slot_ids(routes, capacity, experts):
    batch_size, rows_each, top_count = routes.shape
    flat_ids = routes.reshape(batch_size, rows_each * top_count)
    onehot = (flat_ids[:, :, None] == jnp.arange(experts, dtype=jnp.int32)[None, None, :]).astype(jnp.int32)
    earlier = jnp.cumsum(onehot, axis=1) - onehot
    rank_in = lax.optimization_barrier(jnp.sum(earlier * onehot, axis=2))
    return (flat_ids * capacity + rank_in).reshape(batch_size, rows_each, top_count)

def reference(residual_in, queries, key_rows, value_rows, out_gate, decay_logit, head_gain, w_out, ffn_gain, routing, route_weight, w_gate, w_up, w_down):
    groups = TOKEN_COUNT // TOK_DEV

    def grouped(array, head_width):
        shaped = array.astype(jnp.float32).reshape(groups, TOK_DEV // BLOCK, BLOCK, HEADS, head_width)
        return shaped.transpose(0, 1, 3, 2, 4)
    query_grp = grouped(queries, DK) * DK ** (-0.5)
    key_grp = grouped(key_rows, DK)
    value_grp = grouped(value_rows, DV)
    logdecay_grp = grouped(jax.nn.log_sigmoid(decay_logit) / DECAY_TEMP, DK)

    def through(recurrent_state, inputs):
        current_query, key_now, value_now, decay_now = inputs
        inner_part, query_dec, contrib, passing = block_parts(current_query, key_now, value_now, decay_now)
        readouts, final_state = carry_blocks(query_dec, contrib, passing, recurrent_state)
        return (final_state, inner_part + readouts)
    _, outputs = lax.scan(through, jnp.zeros((HEADS, DK, DV), jnp.float32), (query_grp, key_grp, value_grp, logdecay_grp))
    mixed_out = finish_heads(outputs.reshape(TOKEN_COUNT // BLOCK, HEADS, BLOCK, DV), head_gain, out_gate)
    projected = jnp.dot(mixed_out, w_out, preferred_element_type=jnp.float32)
    residual = (residual_in.astype(jnp.float32) + projected).astype(jnp.bfloat16)
    normed = norm_rows(residual, ffn_gain)
    blocks = TOKEN_COUNT // QROWS
    ranked = slot_ids(routing.reshape(blocks, QROWS, TOP), CAP, EXPERTS).reshape(blocks, QROWS * TOP)
    flat_expert = routing.reshape(blocks, QROWS * TOP)
    rank_in = ranked - flat_expert * CAP
    placed = (flat_expert * (blocks * CAP) + jnp.arange(blocks, dtype=jnp.int32)[:, None] * CAP + rank_in).reshape(-1)
    token_of = jnp.repeat(jnp.arange(TOKEN_COUNT, dtype=jnp.int32), TOP)
    slots_all = EXPERTS * blocks * CAP
    token_table = jnp.zeros((slots_all,), jnp.int32).at[placed].set(token_of).reshape(EXPERTS, blocks * CAP)
    weight_table = jnp.zeros((slots_all,), jnp.float32).at[placed].set(route_weight.reshape(-1)).reshape(EXPERTS, blocks * CAP)
    live_slot = jnp.zeros((slots_all,), jnp.float32).at[placed].set(1.0).reshape(EXPERTS, blocks * CAP)
    part_width = FF // N_TP

    def serve_expert(accumulated, inputs):
        token_ids, slot_weight, slot_live, gate_cols, up_cols, down_rows = inputs
        gathered = jnp.where(slot_live[:, None] > 0, normed[token_ids], jnp.zeros((), jnp.bfloat16))
        gate_pre = jnp.dot(gathered, gate_cols, preferred_element_type=jnp.float32)
        up_pre = jnp.dot(gathered, up_cols, preferred_element_type=jnp.float32)
        hidden = clamped_unit(gate_pre, up_pre).astype(jnp.bfloat16)
        expert_out = jnp.zeros((gathered.shape[0], D), jnp.float32)
        for shard_no in range(N_TP):
            portion = jnp.dot(hidden[:, shard_no * part_width:(shard_no + 1) * part_width], down_rows[shard_no * part_width:(shard_no + 1) * part_width], preferred_element_type=jnp.float32).astype(jnp.bfloat16)
            portion = lax.optimization_barrier(portion)
            expert_out = expert_out + portion.astype(jnp.float32)
        expert_out = expert_out.astype(jnp.bfloat16)
        return (accumulated.at[token_ids].add(slot_weight[:, None] * expert_out.astype(jnp.float32)), None)
    routed, _ = lax.scan(serve_expert, jnp.zeros((TOKEN_COUNT, D), jnp.float32), (token_table, weight_table, live_slot, w_gate, w_up, w_down))
    return (residual.astype(jnp.float32) + routed).astype(jnp.bfloat16)
```

```python
import jax
import jax.numpy as jnp
from jax import lax
from jax.experimental import pallas as pl
from jax.experimental.pallas import tpu as pltpu
from jax.sharding import PartitionSpec as P
import functools

DK = 64
DV = 128


DECAY_TEMP = 16.0
CLAMP_LIMIT = 7.0
SIGMOID_SLOPE = 1.702
NORM_EPS = 1e-06
EXACT_PRECISION = lax.Precision.HIGHEST


def clamped_unit(gate_pre, up_pre):
    gate_cut = jnp.minimum(gate_pre, CLAMP_LIMIT)
    up_cut = jnp.clip(up_pre, -CLAMP_LIMIT, CLAMP_LIMIT)
    return (up_cut + 1.0) * (gate_cut * jax.nn.sigmoid(SIGMOID_SLOPE * gate_cut))


MESH = pl.DeviceIdType.MESH
LANES = 128
SUB = 32
EXP_CAP = 64.0


def nt_dot(left, right):
    return lax.dot_general(
        left, right, (((1,), (1,)), ((), ())), preferred_element_type=jnp.float32
    )


def tn_dot(left, right):
    return lax.dot_general(
        left, right, (((0,), (0,)), ((), ())), preferred_element_type=jnp.float32
    )


def mix_kernel(
    sp_count, tp_count,
    q_ref, k_ref, v_ref, gate_ref, decay_ref, head_gain_ref, w_hbm, ffn_gain_ref,
    routing_ref, weight_ref, res_in_ref,
    res_ref, ext_ref,
    states, attended, mixed, mixed_in, w_vmem,
    w_sem, state_send, state_recv, mix_send, mix_recv,
):
    sp_me, tp_me = lax.axis_index("sp"), lax.axis_index("tp")
    barrier = pltpu.get_barrier_semaphore()

    @pl.loop(1, sp_count)
    def _(d):
        pl.semaphore_signal(
            barrier, inc=1, device_id={"sp": lax.rem(sp_me + d, sp_count)}, device_id_type=MESH
        )

    @pl.loop(1, tp_count)
    def _(d):
        pl.semaphore_signal(
            barrier, inc=1, device_id={"tp": lax.rem(tp_me + d, tp_count)}, device_id_type=MESH
        )

    w_copy = pltpu.make_async_copy(w_hbm, w_vmem, w_sem)
    w_copy.start()

    tokens, key_lanes = q_ref.shape
    value_lanes = v_ref.shape[1]
    head_count = key_lanes // DK
    lane_head = lax.broadcasted_iota(jnp.int32, (1, key_lanes), 1) // DK
    logit = decay_ref[...]
    log_decay = (jnp.minimum(logit, 0.0) - jnp.log1p(jnp.exp(-jnp.abs(logit)))) / DECAY_TEMP
    row_id = lax.broadcasted_iota(jnp.int32, (tokens, tokens), 0)
    col_id = lax.broadcasted_iota(jnp.int32, (tokens, tokens), 1)
    lower = (row_id >= col_id).astype(jnp.float32)
    cumulative = jnp.dot(
        lower, log_decay, precision=EXACT_PRECISION, preferred_element_type=jnp.float32
    )
    keys = k_ref[...].astype(jnp.float32)
    query = q_ref[...].astype(jnp.float32) * DK ** (-0.5)
    values = v_ref[...]
    ending = cumulative[tokens - 1 :, :]
    wide = tn_dot(values, (keys * jnp.exp(ending - cumulative)).astype(jnp.bfloat16))
    state = jnp.zeros((DV, key_lanes), jnp.float32)
    for h in range(head_count):
        state = jnp.where(lane_head == h, wide[h * DV : (h + 1) * DV, :], state)
    passing = jnp.exp(ending)
    passing_hi = passing.astype(jnp.bfloat16).astype(jnp.float32)
    tail_row = lax.broadcasted_iota(jnp.int32, (16, key_lanes), 0)
    tail = jnp.where(
        tail_row == 0, passing_hi, jnp.where(tail_row == 1, passing - passing_hi, 0.0)
    )
    states[sp_me, 0:DV, :] = state.astype(jnp.bfloat16)
    states[sp_me, DV : DV + 16, :] = tail.astype(jnp.bfloat16)

    pl.semaphore_wait(barrier, sp_count + tp_count - 2)

    def state_copy(slot, d):
        return pltpu.make_async_remote_copy(
            src_ref=states.at[slot],
            dst_ref=states.at[slot],
            send_sem=state_send.at[d],
            recv_sem=state_recv.at[slot],
            device_id={"sp": lax.rem(sp_me + d, sp_count)},
            device_id_type=MESH,
        )

    @pl.loop(1, sp_count)
    def _(d):
        state_copy(sp_me, d).start()

    for i in range(tokens // SUB):
        first = i * SUB
        reach = min(-(-(first + SUB) // LANES) * LANES, tokens)
        start = cumulative[first - 1 : first, :] if i else jnp.zeros((1, key_lanes), jnp.float32)
        q_sub = query[first : first + SUB] * jnp.exp(cumulative[first : first + SUB] - start)
        k_sub = keys[:reach] * jnp.exp(jnp.minimum(start - cumulative[:reach], EXP_CAP))
        stacked = jnp.concatenate(
            [jnp.where(lane_head == h, q_sub, 0.0) for h in range(head_count)], axis=0
        )
        scores = nt_dot(stacked.astype(jnp.bfloat16), k_sub.astype(jnp.bfloat16))
        at_row = lax.broadcasted_iota(jnp.int32, scores.shape, 0) % SUB + first
        at_col = lax.broadcasted_iota(jnp.int32, scores.shape, 1)
        scores = jnp.where(at_row >= at_col, scores, 0.0).astype(jnp.bfloat16)
        inner = jnp.dot(scores, values[:reach], preferred_element_type=jnp.float32)
        for h in range(head_count):
            attended[first : first + SUB, h * DV : (h + 1) * DV] = inner[
                h * SUB : (h + 1) * SUB, h * DV : (h + 1) * DV
            ]

    @pl.loop(1, sp_count)
    def _(d):
        state_copy(lax.rem(sp_me + d, sp_count), d).wait_recv()

    def absorb(j, incoming):
        decay = states[j, DV : DV + 16, :].astype(jnp.float32)
        total = decay[0:1, :] + decay[1:2, :]
        following = total * incoming + states[j, 0:DV, :].astype(jnp.float32)
        return jnp.where(j < sp_me, following, incoming)

    incoming = lax.fori_loop(
        0, sp_count, absorb, jnp.zeros((DV, key_lanes), jnp.float32)
    ).astype(jnp.bfloat16)
    query_dec = query * jnp.exp(cumulative)
    for h in range(head_count):
        cols = slice(h * DV, (h + 1) * DV)
        readout = nt_dot(jnp.where(lane_head == h, query_dec, 0.0).astype(jnp.bfloat16), incoming)
        head = attended[:, cols] + readout
        scale = lax.rsqrt(jnp.mean(head * head, axis=-1, keepdims=True) + NORM_EPS)
        opened = gate_ref[:, cols].astype(jnp.float32)
        opened = opened * jax.nn.sigmoid(opened)
        mixed[:, cols] = (head * scale * head_gain_ref[...].astype(jnp.float32) * opened).astype(
            jnp.bfloat16
        )

    rows = res_in_ref.shape[0]

    def mix_copy(block, slot, d):
        return pltpu.make_async_remote_copy(
            src_ref=mixed.at[pl.ds(pl.multiple_of(block * rows, rows), rows)],
            dst_ref=mixed_in.at[slot],
            send_sem=mix_send.at[d],
            recv_sem=mix_recv.at[slot],
            device_id={"tp": lax.rem(tp_me + d, tp_count)},
            device_id_type=MESH,
        )

    for d in range(1, tp_count):
        mix_copy(lax.rem(tp_me + d, tp_count), tp_me, d).start()

    lane = lax.broadcasted_iota(jnp.int32, (rows, LANES), 1)
    named = routing_ref[pl.ds(pl.multiple_of(tp_me * rows, rows), rows), :]
    share = jnp.zeros((rows, LANES), jnp.float32)
    for j in range(weight_ref.shape[1]):
        share = share + jnp.where(
            lane % (LANES // 2) == named[:, j : j + 1], weight_ref[:, j : j + 1], 0.0
        )
    share_hi = share.astype(jnp.bfloat16).astype(jnp.float32)
    width = res_in_ref.shape[1]
    ext_ref[:, width:] = jnp.where(lane < LANES // 2, share_hi, share - share_hi).astype(
        jnp.bfloat16
    )

    w_copy.wait()

    def w_rows(j):
        return w_vmem[pl.ds(pl.multiple_of(j * value_lanes, value_lanes), value_lanes), :]

    projected = jnp.dot(
        mixed[pl.ds(pl.multiple_of(tp_me * rows, rows), rows), :],
        w_rows(tp_me),
        preferred_element_type=jnp.float32,
    )
    for d in range(1, tp_count):
        slot = lax.rem(tp_me + d, tp_count)
        mix_copy(slot, slot, d).wait_recv()
        projected = projected + jnp.dot(
            mixed_in[slot], w_rows(slot), preferred_element_type=jnp.float32
        )
    residual = (res_in_ref[...].astype(jnp.float32) + projected).astype(jnp.bfloat16)
    res_ref[...] = residual
    wide_res = residual.astype(jnp.float32)
    inv = lax.rsqrt(jnp.mean(wide_res * wide_res, axis=-1, keepdims=True) + NORM_EPS)
    ext_ref[:, :width] = (wide_res * inv * ffn_gain_ref[...].astype(jnp.float32)).astype(
        jnp.bfloat16
    )

    @pl.loop(1, sp_count)
    def _(d):
        state_copy(sp_me, d).wait_send()

    for d in range(1, tp_count):
        mix_copy(lax.rem(tp_me + d, tp_count), tp_me, d).wait_send()


def mix_rows(
    queries, key_rows, value_rows, out_gate, decay_logit, head_gain, w_out,
    ffn_gain, routing, route_weight, residual_in,
):
    sp_count, tp_count = lax.axis_size("sp"), lax.axis_size("tp")
    rows, width = residual_in.shape
    tokens, key_lanes = queries.shape
    value_lanes = value_rows.shape[1]
    vmem = pl.BlockSpec(memory_space=pltpu.VMEM)
    return pl.pallas_call(
        functools.partial(mix_kernel, sp_count, tp_count),
        out_shape=(
            jax.ShapeDtypeStruct((rows, width), jnp.bfloat16),
            jax.ShapeDtypeStruct((rows, width + LANES), jnp.bfloat16),
        ),
        in_specs=[vmem] * 6 + [pl.BlockSpec(memory_space=pl.ANY)] + [vmem] * 4,
        out_specs=(vmem, vmem),
        scratch_shapes=[
            pltpu.VMEM((sp_count, DV + 16, key_lanes), jnp.bfloat16),
            pltpu.VMEM((tokens, value_lanes), jnp.float32),
            pltpu.VMEM((tokens, value_lanes), jnp.bfloat16),
            pltpu.VMEM((tp_count, rows, value_lanes), jnp.bfloat16),
            pltpu.VMEM(w_out.shape, jnp.bfloat16),
            pltpu.SemaphoreType.DMA,
            pltpu.SemaphoreType.DMA((sp_count,)),
            pltpu.SemaphoreType.DMA((sp_count,)),
            pltpu.SemaphoreType.DMA((tp_count,)),
            pltpu.SemaphoreType.DMA((tp_count,)),
        ],
        compiler_params=pltpu.CompilerParams(
            collective_id=0, has_side_effects=True, vmem_limit_bytes=40 << 20
        ),
        name="mix_rows",
    )(
        queries, key_rows, value_rows, out_gate, decay_logit, head_gain.reshape(1, -1), w_out,
        ffn_gain.reshape(1, -1), routing, route_weight, residual_in,
    )


GROUP = 16
SPREAD = ("zxy", "zyx", "xzy", "yzx")
GATHER_LAG = (0, 2, 4, 7, 8)
REDUCE_LAG = (0, 1, 3, 6, 8)
REDUCE_AT = 13


def layer_kernel(
    sp_count, tp_count, cuts,
    q_hbm, k_hbm, v_hbm, gate_hbm, decay_hbm, head_gain_hbm, w_out_hbm, ffn_gain_hbm,
    routing_hbm, weight_hbm, res_in_hbm, up_gate_hbm, up_hbm, down_hbm,
    out_ref,
    q_ref, k_ref, v_ref, gate_ref, decay_ref, head_gain_ref, ffn_gain_ref,
    routing_ref, weight_ref, res_ref,
    states, attended, opened, mixed, mixed_in, w_vmem,
    rows_all, share_all, gate_w, up_w, down_w, hidden, parts, got_core, got_one, got_two, got_mid, got_last,
    in_sem, w_sem, state_send, state_recv, mix_send, mix_recv,
    share_send, share_recv, gather_send, gather_recv, reduce_send, reduce_recv,
):
    sp_me, tp_me = lax.axis_index("sp"), lax.axis_index("tp")
    z_count = sp_count // 2
    z, x = sp_me // 2, lax.rem(sp_me, 2)
    y, c = tp_me // 2, lax.rem(tp_me, 2)
    barrier = pltpu.get_barrier_semaphore()

    @pl.loop(1, sp_count)
    def _(d):
        pl.semaphore_signal(
            barrier, inc=1, device_id={"sp": lax.rem(sp_me + d, sp_count)}, device_id_type=MESH
        )

    @pl.loop(1, tp_count)
    def _(d):
        pl.semaphore_signal(
            barrier, inc=1, device_id={"tp": lax.rem(tp_me + d, tp_count)}, device_id_type=MESH
        )

    small = [
        pltpu.make_async_copy(src, dst, in_sem.at[i])
        for i, (src, dst) in enumerate(
            (
                (decay_hbm, decay_ref), (k_hbm, k_ref), (v_hbm, v_ref), (q_hbm, q_ref),
                (routing_hbm, routing_ref), (weight_hbm, weight_ref), (gate_hbm, gate_ref),
                (head_gain_hbm, head_gain_ref), (ffn_gain_hbm, ffn_gain_ref), (res_in_hbm, res_ref),
            )
        )
    ]
    large = [
        pltpu.make_async_copy(src, dst, w_sem.at[i])
        for i, (src, dst) in enumerate(
            ((w_out_hbm, w_vmem), (up_gate_hbm, gate_w), (up_hbm, up_w), (down_hbm, down_w))
        )
    ]
    for load in small + large:
        load.start()

    def remote(src, dst, send, recv, target):
        return pltpu.make_async_remote_copy(
            src_ref=src, dst_ref=dst, send_sem=send, recv_sem=recv,
            device_id=target, device_id_type=MESH,
        )

    partner = {
        "x": {"sp": z * 2 + 1 - x},
        "y": {"tp": (1 - y) * 2 + c},
        "c": {"tp": y * 2 + 1 - c},
    }

    def z_peer(d):
        return {"sp": lax.rem(z + d, z_count) * 2 + x}

    tokens, key_lanes = q_ref.shape
    value_lanes = v_ref.shape[1]
    rows, width = res_ref.shape
    head_count = key_lanes // DK
    lane_head = lax.broadcasted_iota(jnp.int32, (1, key_lanes), 1) // DK
    small[0].wait()
    logit = decay_ref[...]
    log_decay = (jnp.minimum(logit, 0.0) - jnp.log1p(jnp.exp(-jnp.abs(logit)))) / DECAY_TEMP
    row_id = lax.broadcasted_iota(jnp.int32, (tokens, tokens), 0)
    col_id = lax.broadcasted_iota(jnp.int32, (tokens, tokens), 1)
    lower = (row_id >= col_id).astype(jnp.float32)
    cumulative = jnp.dot(
        lower, log_decay, precision=EXACT_PRECISION, preferred_element_type=jnp.float32
    )
    for load in small[1:]:
        load.wait()
    keys = k_ref[...].astype(jnp.float32)
    query = q_ref[...].astype(jnp.float32) * DK ** (-0.5)
    values = v_ref[...]
    ending = cumulative[tokens - 1 :, :]
    wide = tn_dot(values, (keys * jnp.exp(ending - cumulative)).astype(jnp.bfloat16))
    state = jnp.zeros((DV, key_lanes), jnp.float32)
    for h in range(head_count):
        state = jnp.where(lane_head == h, wide[h * DV : (h + 1) * DV, :], state)
    passing = jnp.exp(ending)
    passing_hi = passing.astype(jnp.bfloat16).astype(jnp.float32)
    tail_row = lax.broadcasted_iota(jnp.int32, (16, key_lanes), 0)
    tail = jnp.where(
        tail_row == 0, passing_hi, jnp.where(tail_row == 1, passing - passing_hi, 0.0)
    )
    states[sp_me, 0:DV, :] = state.astype(jnp.bfloat16)
    states[sp_me, DV : DV + 16, :] = tail.astype(jnp.bfloat16)

    pl.semaphore_wait(barrier, sp_count + tp_count - 2)

    def state_copy(slot, d):
        return remote(
            states.at[slot], states.at[slot], state_send.at[d], state_recv.at[slot],
            {"sp": sp_me + d},
        )

    @pl.loop(1, sp_count - sp_me)
    def _(d):
        state_copy(sp_me, d).start()

    lane = lax.broadcasted_iota(jnp.int32, (LANES, tokens), 0)
    share = jnp.zeros((LANES, tokens), jnp.float32)
    spot = lax.broadcasted_iota(jnp.int32, (rows, tokens), 1)
    mine = spot == lax.broadcasted_iota(jnp.int32, (rows, tokens), 0) + tp_me * rows
    for j in range(weight_ref.shape[0]):
        weight = jnp.concatenate([weight_ref[j : j + 1, :]] * tp_count, axis=1)
        share = share + jnp.where(lane % (LANES // 2) == routing_ref[j : j + 1, :], weight, 0.0)
    share_hi = share.astype(jnp.bfloat16).astype(jnp.float32)
    share = jnp.where(lane < LANES // 2, share_hi, share - share_hi).astype(jnp.bfloat16)
    share_all[z, x, y, c] = nt_dot(mine.astype(jnp.bfloat16), share).astype(jnp.bfloat16)

    def spread(ref, lead, cols, order, stage, arriving, send, recv):
        at = {"z": z, "x": x, "y": y, "c": c}
        for axis in order[:stage]:
            at[axis] = slice(None)
        axis = order[stage]

        def block(place):
            return ref.at[(*lead, place["z"], place["x"], place["y"], place["c"], slice(None), cols)]

        copies = []
        if axis == "z":
            for d in range(1, z_count):
                src = block({**at, "z": lax.rem(z + z_count - d, z_count)} if arriving else at)
                copies.append(remote(src, src, send(d - 1), recv(d - 1), z_peer(d)))
            return copies
        slot = z_count - 1 + "xyc".index(axis)
        src = block({**at, axis: 1 - at[axis]} if arriving else at)
        return [remote(src, src, send(slot), recv(slot), partner[axis])]

    def share_copies(stage, arriving):
        return spread(
            share_all, (), slice(None), "zxyc", stage, arriving,
            lambda i: share_send.at[i], lambda i: share_recv.at[i],
        )

    def share_step(stage):
        if stage:
            for copy in share_copies(stage - 1, True):
                copy.wait_recv()
        if stage < 4:
            for copy in share_copies(stage, False):
                copy.start()

    share_step(0)

    for i in range(tokens // SUB):
        first = i * SUB
        reach = min(-(-(first + SUB) // LANES) * LANES, tokens)
        start = cumulative[first - 1 : first, :] if i else jnp.zeros((1, key_lanes), jnp.float32)
        q_sub = query[first : first + SUB] * jnp.exp(cumulative[first : first + SUB] - start)
        k_sub = keys[:reach] * jnp.exp(jnp.minimum(start - cumulative[:reach], EXP_CAP))
        stacked = jnp.concatenate(
            [jnp.where(lane_head == h, q_sub, 0.0) for h in range(head_count)], axis=0
        )
        scores = nt_dot(stacked.astype(jnp.bfloat16), k_sub.astype(jnp.bfloat16))
        at_row = lax.broadcasted_iota(jnp.int32, scores.shape, 0) % SUB + first
        at_col = lax.broadcasted_iota(jnp.int32, scores.shape, 1)
        scores = jnp.where(at_row >= at_col, scores, 0.0).astype(jnp.bfloat16)
        inner = jnp.dot(scores, values[:reach], preferred_element_type=jnp.float32)
        for h in range(head_count):
            attended[first : first + SUB, h * DV : (h + 1) * DV] = inner[
                h * SUB : (h + 1) * SUB, h * DV : (h + 1) * DV
            ]
    for h in range(head_count):
        cols = slice(h * DV, (h + 1) * DV)
        wide_gate = gate_ref[:, cols].astype(jnp.float32)
        opened[:, cols] = (
            head_gain_ref[...].astype(jnp.float32) * wide_gate * jax.nn.sigmoid(wide_gate)
        )
    share_step(1)

    @pl.loop(0, sp_me)
    def _(j):
        state_copy(j, 0).wait_recv()

    def absorb(j, incoming):
        decay = states[j, DV : DV + 16, :].astype(jnp.float32)
        total = decay[0:1, :] + decay[1:2, :]
        return total * incoming + states[j, 0:DV, :].astype(jnp.float32)

    incoming = lax.fori_loop(
        0, sp_me, absorb, jnp.zeros((DV, key_lanes), jnp.float32)
    ).astype(jnp.bfloat16)
    query_dec = query * jnp.exp(cumulative)
    for h in range(head_count):
        cols = slice(h * DV, (h + 1) * DV)
        readout = nt_dot(jnp.where(lane_head == h, query_dec, 0.0).astype(jnp.bfloat16), incoming)
        head = attended[:, cols] + readout
        scale = lax.rsqrt(jnp.mean(head * head, axis=-1, keepdims=True) + NORM_EPS)
        mixed[:, cols] = (head * scale * opened[:, cols]).astype(jnp.bfloat16)

    def mix_copy(block, slot, d):
        return remote(
            mixed.at[pl.ds(pl.multiple_of(block * rows, rows), rows)], mixed_in.at[slot],
            mix_send.at[d], mix_recv.at[slot], {"tp": lax.rem(tp_me + d, tp_count)},
        )

    for d in range(1, tp_count):
        mix_copy(lax.rem(tp_me + d, tp_count), tp_me, d).start()
    share_step(2)
    large[0].wait()

    def w_rows(j):
        return w_vmem[pl.ds(pl.multiple_of(j * value_lanes, value_lanes), value_lanes), :]

    projected = jnp.dot(
        mixed[pl.ds(pl.multiple_of(tp_me * rows, rows), rows), :],
        w_rows(tp_me),
        preferred_element_type=jnp.float32,
    )
    for d in range(1, tp_count):
        slot = lax.rem(tp_me + d, tp_count)
        mix_copy(slot, slot, d).wait_recv()
        projected = projected + jnp.dot(
            mixed_in[slot], w_rows(slot), preferred_element_type=jnp.float32
        )
    residual = (res_ref[...].astype(jnp.float32) + projected).astype(jnp.bfloat16)
    res_ref[...] = residual
    wide_res = residual.astype(jnp.float32)
    inv = lax.rsqrt(jnp.mean(wide_res * wide_res, axis=-1, keepdims=True) + NORM_EPS)
    groups = rows // GROUP
    for k in range(width // LANES):
        cols = slice(k * LANES, (k + 1) * LANES)
        normed = wide_res[:, cols] * inv * ffn_gain_ref[k : k + 1, :].astype(jnp.float32)
        normed = normed.astype(jnp.bfloat16)
        for g in range(groups):
            rows_all[g, z, x, y, c, :, cols] = normed[g * GROUP : (g + 1) * GROUP]

    chunks = len(SPREAD)

    def span(q):
        return pl.ds(cuts[q][0], cuts[q][1])

    def gather_copies(g, q, stage, arriving):
        return spread(
            rows_all, (g,), span(q), SPREAD[q] + "c", stage, arriving,
            lambda i: gather_send.at[g, q, i], lambda i: gather_recv.at[g, q, i],
        )

    def gather_step(g, q, stage):
        if stage:
            for copy in gather_copies(g, q, stage - 1, True):
                copy.wait_recv()
        if stage < 4:
            for copy in gather_copies(g, q, stage, False):
                copy.start()

    group_rows = sp_count * tp_count * GROUP
    half_rows = group_rows // 2
    half_z = z_count // 2

    def raise_half(g, half):
        zs = slice(half * half_z, (half + 1) * half_z)
        block = rows_all[g, zs].reshape(half_rows, width)
        gate_pre = jnp.dot(block, gate_w[...], preferred_element_type=jnp.float32)
        up_pre = jnp.dot(block, up_w[...], preferred_element_type=jnp.float32)
        tags = share_all[zs, :, :, :, pl.ds(pl.multiple_of(g * GROUP, GROUP), GROUP), :]
        tags = tags.reshape(half_rows, LANES).astype(jnp.float32)
        lane = lax.broadcasted_iota(jnp.int32, (half_rows, LANES), 1) % (LANES // 2)
        share = jnp.sum(jnp.where(lane == sp_me, tags, 0.0), axis=-1, keepdims=True)
        hidden[g, half * half_rows : (half + 1) * half_rows] = (
            clamped_unit(gate_pre, up_pre) * share
        ).astype(jnp.bfloat16)

    def lower_chunk(g, q):
        at, size = cuts[q]
        out = jnp.dot(hidden[g], down_w[:, at : at + size], preferred_element_type=jnp.float32)
        parts[g, :, :, :, :, :, at : at + size] = out.astype(jnp.bfloat16).reshape(
            z_count, 2, 2, 2, GROUP, size
        )

    every = slice(None)

    def reduce_order(q):
        return "c" + SPREAD[q][::-1]

    def reduce_copies(g, q, stage):
        order, cols = reduce_order(q), span(q)
        at = {"z": every, "x": every, "y": every, "c": every}
        for axis in order[:stage]:
            at[axis] = {"z": z, "x": x, "y": y, "c": c}[axis]
        axis = order[stage]

        def block(place):
            return parts.at[g, place["z"], place["x"], place["y"], place["c"], :, cols]

        if axis == "z":
            copies = []
            for d in range(1, z_count):
                dst = got_mid.at[g, d - 1, :, :, cols] if stage == 2 else got_last.at[g, d - 1, :, cols]
                copies.append(
                    remote(
                        block({**at, "z": lax.rem(z + d, z_count)}), dst,
                        reduce_send.at[g, q, d - 1], reduce_recv.at[g, q, d - 1], z_peer(d),
                    )
                )
            return copies
        own = {"x": x, "y": y, "c": c}[axis]
        dst = (
            got_core.at[g, :, :, :, :, cols] if stage == 0
            else got_one.at[g, :, :, :, cols] if stage == 1
            else got_two.at[g, :, :, cols] if stage == 2
            else got_last.at[g, 0, :, cols]
        )
        slot = z_count - 1 + "xyc".index(axis)
        return [
            remote(
                block({**at, axis: 1 - own}), dst,
                reduce_send.at[g, q, slot], reduce_recv.at[g, q, slot], partner[axis],
            )
        ]

    def f32(value):
        return value.astype(jnp.float32)

    def absorb_step(g, q, stage):
        for copy in reduce_copies(g, q, stage):
            copy.wait_recv()
        order = reduce_order(q)
        at, size = cuts[q]
        cols = slice(at, at + size)
        if stage == 0:
            @pl.loop(0, z_count)
            def _(zz):
                ours = parts[g, zz, :, :, c, :, cols]
                parts[g, zz, :, :, c, :, cols] = (
                    f32(ours) + f32(got_core[g, zz, :, :, :, cols])
                ).astype(jnp.bfloat16)
        elif stage == 1:
            where = (g, every, x, every, c) if order[1] == "x" else (g, every, every, y, c)
            where = (*where, every, cols)
            parts[where] = (f32(parts[where]) + f32(got_one[g, :, :, :, cols])).astype(jnp.bfloat16)
        elif stage == 2 and order[2] != "z":
            where = (g, every, x, y, c, every, cols)
            parts[where] = (f32(parts[where]) + f32(got_two[g, :, :, cols])).astype(jnp.bfloat16)
        elif stage == 2:
            where = (g, z, x, every, c) if order[1] == "x" else (g, z, every, y, c)
            where = (*where, every, cols)
            total = f32(parts[where])
            for d in range(1, z_count):
                total = total + f32(got_mid[g, d - 1, :, :, cols])
            parts[where] = total.astype(jnp.bfloat16)
        else:
            total = f32(parts[g, z, x, y, c, :, cols])
            for d in range(1, z_count if order[3] == "z" else 2):
                total = total + f32(got_last[g, d - 1, :, cols])
            here = pl.ds(pl.multiple_of(g * GROUP, GROUP), GROUP)
            out_ref[here, cols] = (f32(res_ref[here, cols]) + total).astype(jnp.bfloat16)

    def reduce_step(g, q, stage):
        if stage:
            absorb_step(g, q, stage - 1)
        if stage < 4:
            for copy in reduce_copies(g, q, stage):
                copy.start()

    def at_lag(it, q, lag, step):
        g = it + (q - lag) // chunks

        @pl.when((g >= 0) & (g < groups))
        def _():
            step(g, (q - lag) % chunks)

    last = groups * chunks - 1 + REDUCE_AT + REDUCE_LAG[4]
    share_step(3)

    @pl.loop(0, last // chunks + 1)
    def _(it):
        @pl.when(it == 2)
        def _():
            share_step(4)
            for load in large[1:]:
                load.wait()

        for q in range(chunks):
            for stage in (0, 1, 2, 3, 4):
                at_lag(it, q, GATHER_LAG[stage], functools.partial(gather_step, stage=stage))
            if q == chunks - 1:
                at_lag(it, q, GATHER_LAG[4], lambda g, _: raise_half(g, 0))
            if q == 0:
                at_lag(it, q, GATHER_LAG[4] + 1, lambda g, _: raise_half(g, 1))
            at_lag(it, q, REDUCE_AT, lower_chunk)
            for stage in (0, 1, 2, 3, 4):
                at_lag(it, q, REDUCE_AT + REDUCE_LAG[stage], functools.partial(reduce_step, stage=stage))

    @pl.loop(1, sp_count - sp_me)
    def _(d):
        state_copy(sp_me, d).wait_send()

    for d in range(1, tp_count):
        mix_copy(lax.rem(tp_me + d, tp_count), tp_me, d).wait_send()
    for stage in range(4):
        for copy in share_copies(stage, False):
            copy.wait_send()

    @pl.loop(0, groups)
    def _(g):
        for q in range(chunks):
            for stage in range(4):
                for copy in gather_copies(g, q, stage, False):
                    copy.wait_send()
                for copy in reduce_copies(g, q, stage):
                    copy.wait_send()


def column_cuts(width):
    tiles = width // LANES
    edges = [tiles * share // 16 * LANES for share in (0, 5, 10, 13, 16)]
    return [(edges[i], edges[i + 1] - edges[i]) for i in range(4)]


def layer_rows(
    queries, key_rows, value_rows, out_gate, decay_logit, head_gain, w_out,
    ffn_gain, routing, route_weight, residual_in, gate_cols, up_cols, down_rows,
):
    sp_count, tp_count = lax.axis_size("sp"), lax.axis_size("tp")
    rows, width = residual_in.shape
    tokens, key_lanes = queries.shape
    value_lanes = value_rows.shape[1]
    units = gate_cols.shape[1]
    z_count, groups = sp_count // 2, rows // GROUP
    group_rows = sp_count * tp_count * GROUP
    cuts = column_cuts(width)
    hbm = pl.BlockSpec(memory_space=pl.ANY)
    vmem = pl.BlockSpec(memory_space=pltpu.VMEM)
    bf16, f32 = jnp.bfloat16, jnp.float32
    dma = pltpu.SemaphoreType.DMA
    ways = z_count + 2
    operands = (
        queries, key_rows, value_rows, out_gate, decay_logit, head_gain.reshape(1, -1), w_out,
        ffn_gain.reshape(-1, LANES), routing.T, route_weight.T, residual_in,
        gate_cols, up_cols, down_rows,
    )

    def like(array):
        return pltpu.VMEM(array.shape, array.dtype)

    return pl.pallas_call(
        functools.partial(layer_kernel, sp_count, tp_count, cuts),
        out_shape=jax.ShapeDtypeStruct((rows, width), bf16),
        in_specs=[hbm] * len(operands),
        out_specs=vmem,
        scratch_shapes=[
            *(like(operands[i]) for i in (0, 1, 2, 3, 4, 5, 7, 8, 9, 10)),
            pltpu.VMEM((sp_count, DV + 16, key_lanes), bf16),
            pltpu.VMEM((tokens, value_lanes), f32),
            pltpu.VMEM((tokens, value_lanes), f32),
            pltpu.VMEM((tokens, value_lanes), bf16),
            pltpu.VMEM((tp_count, rows, value_lanes), bf16),
            like(w_out),
            pltpu.VMEM((groups, z_count, 2, 2, 2, GROUP, width), bf16),
            pltpu.VMEM((z_count, 2, 2, 2, rows, LANES), bf16),
            like(gate_cols),
            like(up_cols),
            like(down_rows),
            pltpu.VMEM((groups, group_rows, units), bf16),
            pltpu.VMEM((groups, z_count, 2, 2, 2, GROUP, width), bf16),
            pltpu.VMEM((groups, z_count, 2, 2, GROUP, width), bf16),
            pltpu.VMEM((groups, z_count, 2, GROUP, width), bf16),
            pltpu.VMEM((groups, z_count, GROUP, width), bf16),
            pltpu.VMEM((groups, z_count - 1, 2, GROUP, width), bf16),
            pltpu.VMEM((groups, z_count - 1, GROUP, width), bf16),
            dma((10,)),
            dma((4,)),
            dma((sp_count,)),
            dma((sp_count,)),
            dma((tp_count,)),
            dma((tp_count,)),
            dma((ways,)),
            dma((ways,)),
            dma((groups, 4, ways)),
            dma((groups, 4, ways)),
            dma((groups, 4, ways)),
            dma((groups, 4, ways)),
        ],
        compiler_params=pltpu.CompilerParams(
            collective_id=1, has_side_effects=True, vmem_limit_bytes=62 << 20
        ),
        name="layer_rows",
    )(*operands)


def slot_ids(routes, capacity, experts):
    batch_size, rows_each, top_count = routes.shape
    flat_ids = routes.reshape(batch_size, rows_each * top_count)
    onehot = (flat_ids[:, :, None] == jnp.arange(experts, dtype=jnp.int32)[None, None, :]).astype(
        jnp.int32
    )
    earlier = jnp.cumsum(onehot, axis=1) - onehot
    rank_in = jnp.sum(earlier * onehot, axis=2)
    return (flat_ids * capacity + rank_in).reshape(batch_size, rows_each, top_count)


def dispatch_rows(slots, row_data, slot_total):
    chosen = jnp.any(slots[..., None] == jnp.arange(slot_total, dtype=jnp.int32), axis=2).astype(
        jnp.bfloat16
    )
    return jnp.einsum("brs,brd->bsd", chosen, row_data, preferred_element_type=jnp.float32).astype(
        jnp.bfloat16
    )


def on_device(
    residual_in,
    queries,
    key_rows,
    value_rows,
    out_gate,
    decay_logit,
    head_gain,
    w_out,
    ffn_gain,
    routing,
    route_weight,
    w_gate,
    w_up,
    w_down,
):
    tp_count = lax.axis_size("tp")
    experts = lax.axis_size("sp")
    quarter = residual_in.shape[0]
    top_count = routing.shape[1]
    model_width = residual_in.shape[1]
    capacity = 2 * routing.shape[0] * top_count // (tp_count * experts)
    slot_total = experts * capacity
    if (
        capacity >= quarter and experts <= LANES // 2 and experts % 4 == 0
        and tp_count == 4 and quarter % GROUP == 0
    ):
        return layer_rows(
            queries, key_rows, value_rows, out_gate, decay_logit, head_gain, w_out,
            ffn_gain, routing, route_weight, residual_in, w_gate[0], w_up[0], w_down[0],
        )
    residual, extended = mix_rows(
        queries, key_rows, value_rows, out_gate, decay_logit, head_gain, w_out,
        ffn_gain, routing, route_weight, residual_in,
    )
    normed = extended[:, :model_width]
    gate_cols = w_gate[0]
    up_cols = w_up[0]
    down_rows = w_down[0]
    own_routes = lax.dynamic_slice_in_dim(routing, lax.axis_index("tp") * quarter, quarter, 0)
    own_slots = slot_ids(own_routes[None], capacity, experts)[0]
    outgoing = dispatch_rows(own_slots[None], normed[None], slot_total)[0]
    arrived = lax.all_to_all(
        outgoing.reshape(experts, capacity, model_width),
        "sp",
        split_axis=0,
        concat_axis=0,
        tiled=True,
    )
    portion = lax.all_gather(arrived[None], "tp", axis=0, tiled=True)
    flat_rows = portion.reshape(-1, model_width)
    gate_pre = jnp.dot(flat_rows, gate_cols, preferred_element_type=jnp.float32)
    up_pre = jnp.dot(flat_rows, up_cols, preferred_element_type=jnp.float32)
    hidden_rows = clamped_unit(gate_pre, up_pre).astype(jnp.bfloat16)
    hidden = hidden_rows.reshape(portion.shape[:-1] + (gate_cols.shape[1],))
    portion = hidden
    partial_out = jnp.dot(
        portion.reshape(-1, hidden.shape[-1]), down_rows, preferred_element_type=jnp.float32
    ).astype(jnp.bfloat16)
    partial_out = lax.optimization_barrier(partial_out)
    summed = lax.psum_scatter(
        partial_out.astype(jnp.float32)
        .reshape(portion.shape[:-1] + (model_width,))
        .astype(jnp.bfloat16),
        "tp",
        scatter_dimension=0,
        tiled=True,
    ).astype(jnp.float32)
    returned = lax.all_to_all(
        summed[0].astype(jnp.bfloat16), "sp", split_axis=0, concat_axis=0, tiled=True
    )
    picked = jnp.take(
        returned.reshape(slot_total, model_width), own_slots.reshape(-1), axis=0
    ).reshape(quarter, top_count, model_width)
    routed = jnp.sum(picked.astype(jnp.float32) * route_weight[:, :, None], axis=1)
    return (residual.astype(jnp.float32) + routed).astype(jnp.bfloat16)


def solution(mesh):
    placed = (
        P(("sp", "tp"), None),
        P("sp", "tp"),
        P("sp", "tp"),
        P("sp", "tp"),
        P("sp", "tp"),
        P("sp", "tp"),
        P(),
        P(),
        P(),
        P("sp", None),
        P(("sp", "tp"), None),
        P("sp", None, "tp"),
        P("sp", None, "tp"),
        P("sp", "tp", None),
    )
    return jax.shard_map(
        on_device, mesh=mesh, in_specs=placed, out_specs=P(("sp", "tp"), None), check_vma=False
    )
```

```python
import jax
import jax.numpy as jnp
from jax import lax
from jax.experimental import pallas as pl
from jax.experimental.pallas import tpu as pltpu
from jax.sharding import PartitionSpec as P
import functools

DK = 64
DV = 128


DECAY_TEMP = 16.0
CLAMP_LIMIT = 7.0
SIGMOID_SLOPE = 1.702
NORM_EPS = 1e-06
EXACT_PRECISION = lax.Precision.HIGHEST


def clamped_unit(gate_pre, up_pre):
    gate_cut = jnp.minimum(gate_pre, CLAMP_LIMIT)
    up_cut = jnp.clip(up_pre, -CLAMP_LIMIT, CLAMP_LIMIT)
    return (up_cut + 1.0) * (gate_cut * jax.nn.sigmoid(SIGMOID_SLOPE * gate_cut))


MESH = pl.DeviceIdType.MESH
LANES = 128
SUB = 32
EXP_CAP = 64.0


def nt_dot(left, right):
    return lax.dot_general(
        left, right, (((1,), (1,)), ((), ())), preferred_element_type=jnp.float32
    )


def tn_dot(left, right):
    return lax.dot_general(
        left, right, (((0,), (0,)), ((), ())), preferred_element_type=jnp.float32
    )


def mix_kernel(
    sp_count, tp_count,
    q_ref, k_ref, v_ref, gate_ref, decay_ref, head_gain_ref, w_hbm, ffn_gain_ref,
    routing_ref, weight_ref, res_in_ref,
    res_ref, ext_ref,
    states, attended, mixed, mixed_in, w_vmem,
    w_sem, state_send, state_recv, mix_send, mix_recv,
):
    sp_me, tp_me = lax.axis_index("sp"), lax.axis_index("tp")
    barrier = pltpu.get_barrier_semaphore()

    @pl.loop(1, sp_count)
    def _(d):
        pl.semaphore_signal(
            barrier, inc=1, device_id={"sp": lax.rem(sp_me + d, sp_count)}, device_id_type=MESH
        )

    @pl.loop(1, tp_count)
    def _(d):
        pl.semaphore_signal(
            barrier, inc=1, device_id={"tp": lax.rem(tp_me + d, tp_count)}, device_id_type=MESH
        )

    w_copy = pltpu.make_async_copy(w_hbm, w_vmem, w_sem)
    w_copy.start()

    tokens, key_lanes = q_ref.shape
    value_lanes = v_ref.shape[1]
    head_count = key_lanes // DK
    lane_head = lax.broadcasted_iota(jnp.int32, (1, key_lanes), 1) // DK
    logit = decay_ref[...]
    log_decay = (jnp.minimum(logit, 0.0) - jnp.log1p(jnp.exp(-jnp.abs(logit)))) / DECAY_TEMP
    row_id = lax.broadcasted_iota(jnp.int32, (tokens, tokens), 0)
    col_id = lax.broadcasted_iota(jnp.int32, (tokens, tokens), 1)
    lower = (row_id >= col_id).astype(jnp.float32)
    cumulative = jnp.dot(
        lower, log_decay, precision=EXACT_PRECISION, preferred_element_type=jnp.float32
    )
    keys = k_ref[...].astype(jnp.float32)
    query = q_ref[...].astype(jnp.float32) * DK ** (-0.5)
    values = v_ref[...]
    ending = cumulative[tokens - 1 :, :]
    wide = tn_dot(values, (keys * jnp.exp(ending - cumulative)).astype(jnp.bfloat16))
    state = jnp.zeros((DV, key_lanes), jnp.float32)
    for h in range(head_count):
        state = jnp.where(lane_head == h, wide[h * DV : (h + 1) * DV, :], state)
    passing = jnp.exp(ending)
    passing_hi = passing.astype(jnp.bfloat16).astype(jnp.float32)
    tail_row = lax.broadcasted_iota(jnp.int32, (16, key_lanes), 0)
    tail = jnp.where(
        tail_row == 0, passing_hi, jnp.where(tail_row == 1, passing - passing_hi, 0.0)
    )
    states[sp_me, 0:DV, :] = state.astype(jnp.bfloat16)
    states[sp_me, DV : DV + 16, :] = tail.astype(jnp.bfloat16)

    pl.semaphore_wait(barrier, sp_count + tp_count - 2)

    def state_copy(slot, d):
        return pltpu.make_async_remote_copy(
            src_ref=states.at[slot],
            dst_ref=states.at[slot],
            send_sem=state_send.at[d],
            recv_sem=state_recv.at[slot],
            device_id={"sp": lax.rem(sp_me + d, sp_count)},
            device_id_type=MESH,
        )

    @pl.loop(1, sp_count)
    def _(d):
        state_copy(sp_me, d).start()

    for i in range(tokens // SUB):
        first = i * SUB
        reach = min(-(-(first + SUB) // LANES) * LANES, tokens)
        start = cumulative[first - 1 : first, :] if i else jnp.zeros((1, key_lanes), jnp.float32)
        q_sub = query[first : first + SUB] * jnp.exp(cumulative[first : first + SUB] - start)
        k_sub = keys[:reach] * jnp.exp(jnp.minimum(start - cumulative[:reach], EXP_CAP))
        stacked = jnp.concatenate(
            [jnp.where(lane_head == h, q_sub, 0.0) for h in range(head_count)], axis=0
        )
        scores = nt_dot(stacked.astype(jnp.bfloat16), k_sub.astype(jnp.bfloat16))
        at_row = lax.broadcasted_iota(jnp.int32, scores.shape, 0) % SUB + first
        at_col = lax.broadcasted_iota(jnp.int32, scores.shape, 1)
        scores = jnp.where(at_row >= at_col, scores, 0.0).astype(jnp.bfloat16)
        inner = jnp.dot(scores, values[:reach], preferred_element_type=jnp.float32)
        for h in range(head_count):
            attended[first : first + SUB, h * DV : (h + 1) * DV] = inner[
                h * SUB : (h + 1) * SUB, h * DV : (h + 1) * DV
            ]

    @pl.loop(1, sp_count)
    def _(d):
        state_copy(lax.rem(sp_me + d, sp_count), d).wait_recv()

    def absorb(j, incoming):
        decay = states[j, DV : DV + 16, :].astype(jnp.float32)
        total = decay[0:1, :] + decay[1:2, :]
        following = total * incoming + states[j, 0:DV, :].astype(jnp.float32)
        return jnp.where(j < sp_me, following, incoming)

    incoming = lax.fori_loop(
        0, sp_count, absorb, jnp.zeros((DV, key_lanes), jnp.float32)
    ).astype(jnp.bfloat16)
    query_dec = query * jnp.exp(cumulative)
    for h in range(head_count):
        cols = slice(h * DV, (h + 1) * DV)
        readout = nt_dot(jnp.where(lane_head == h, query_dec, 0.0).astype(jnp.bfloat16), incoming)
        head = attended[:, cols] + readout
        scale = lax.rsqrt(jnp.mean(head * head, axis=-1, keepdims=True) + NORM_EPS)
        opened = gate_ref[:, cols].astype(jnp.float32)
        opened = opened * jax.nn.sigmoid(opened)
        mixed[:, cols] = (head * scale * head_gain_ref[...].astype(jnp.float32) * opened).astype(
            jnp.bfloat16
        )

    rows = res_in_ref.shape[0]

    def mix_copy(block, slot, d):
        return pltpu.make_async_remote_copy(
            src_ref=mixed.at[pl.ds(pl.multiple_of(block * rows, rows), rows)],
            dst_ref=mixed_in.at[slot],
            send_sem=mix_send.at[d],
            recv_sem=mix_recv.at[slot],
            device_id={"tp": lax.rem(tp_me + d, tp_count)},
            device_id_type=MESH,
        )

    for d in range(1, tp_count):
        mix_copy(lax.rem(tp_me + d, tp_count), tp_me, d).start()

    lane = lax.broadcasted_iota(jnp.int32, (rows, LANES), 1)
    named = routing_ref[pl.ds(pl.multiple_of(tp_me * rows, rows), rows), :]
    share = jnp.zeros((rows, LANES), jnp.float32)
    for j in range(weight_ref.shape[1]):
        share = share + jnp.where(
            lane % (LANES // 2) == named[:, j : j + 1], weight_ref[:, j : j + 1], 0.0
        )
    share_hi = share.astype(jnp.bfloat16).astype(jnp.float32)
    width = res_in_ref.shape[1]
    ext_ref[:, width:] = jnp.where(lane < LANES // 2, share_hi, share - share_hi).astype(
        jnp.bfloat16
    )

    w_copy.wait()

    def w_rows(j):
        return w_vmem[pl.ds(pl.multiple_of(j * value_lanes, value_lanes), value_lanes), :]

    projected = jnp.dot(
        mixed[pl.ds(pl.multiple_of(tp_me * rows, rows), rows), :],
        w_rows(tp_me),
        preferred_element_type=jnp.float32,
    )
    for d in range(1, tp_count):
        slot = lax.rem(tp_me + d, tp_count)
        mix_copy(slot, slot, d).wait_recv()
        projected = projected + jnp.dot(
            mixed_in[slot], w_rows(slot), preferred_element_type=jnp.float32
        )
    residual = (res_in_ref[...].astype(jnp.float32) + projected).astype(jnp.bfloat16)
    res_ref[...] = residual
    wide_res = residual.astype(jnp.float32)
    inv = lax.rsqrt(jnp.mean(wide_res * wide_res, axis=-1, keepdims=True) + NORM_EPS)
    ext_ref[:, :width] = (wide_res * inv * ffn_gain_ref[...].astype(jnp.float32)).astype(
        jnp.bfloat16
    )

    @pl.loop(1, sp_count)
    def _(d):
        state_copy(sp_me, d).wait_send()

    for d in range(1, tp_count):
        mix_copy(lax.rem(tp_me + d, tp_count), tp_me, d).wait_send()


def mix_rows(
    queries, key_rows, value_rows, out_gate, decay_logit, head_gain, w_out,
    ffn_gain, routing, route_weight, residual_in,
):
    sp_count, tp_count = lax.axis_size("sp"), lax.axis_size("tp")
    rows, width = residual_in.shape
    tokens, key_lanes = queries.shape
    value_lanes = value_rows.shape[1]
    vmem = pl.BlockSpec(memory_space=pltpu.VMEM)
    return pl.pallas_call(
        functools.partial(mix_kernel, sp_count, tp_count),
        out_shape=(
            jax.ShapeDtypeStruct((rows, width), jnp.bfloat16),
            jax.ShapeDtypeStruct((rows, width + LANES), jnp.bfloat16),
        ),
        in_specs=[vmem] * 6 + [pl.BlockSpec(memory_space=pl.ANY)] + [vmem] * 4,
        out_specs=(vmem, vmem),
        scratch_shapes=[
            pltpu.VMEM((sp_count, DV + 16, key_lanes), jnp.bfloat16),
            pltpu.VMEM((tokens, value_lanes), jnp.float32),
            pltpu.VMEM((tokens, value_lanes), jnp.bfloat16),
            pltpu.VMEM((tp_count, rows, value_lanes), jnp.bfloat16),
            pltpu.VMEM(w_out.shape, jnp.bfloat16),
            pltpu.SemaphoreType.DMA,
            pltpu.SemaphoreType.DMA((sp_count,)),
            pltpu.SemaphoreType.DMA((sp_count,)),
            pltpu.SemaphoreType.DMA((tp_count,)),
            pltpu.SemaphoreType.DMA((tp_count,)),
        ],
        compiler_params=pltpu.CompilerParams(
            collective_id=0, has_side_effects=True, vmem_limit_bytes=40 << 20
        ),
        name="mix_rows",
    )(
        queries, key_rows, value_rows, out_gate, decay_logit, head_gain.reshape(1, -1), w_out,
        ffn_gain.reshape(1, -1), routing, route_weight, residual_in,
    )


GROUP = 16
PIECES = (('zxy', 5), ('zyx', 5), ('xzy', 3), ('yzx', 3))
SPREAD = tuple(order for order, _ in PIECES)
GATHER_PACE, REDUCE_PACE, RAISE_GAP = 5.93, 0.99, 0.74
GATHER_AT = ((-0.39, 3.6, 7.61, 22.71, 27.52), (-0.09, 7.59, 11.49, 18.04, 27.81), (-10.56, 9.95, 16.61, 26.65, 28.74), (-4.53, 8.4, 15.26, 20.77, 24.71))
REDUCE_AT = ((0.0, 1.36, 6.01, 10.78, 26.83), (0.43, 4.07, 10.15, 15.03, 38.01), (0.86, 3.15, 8.38, 17.57, 24.05), (1.29, 3.51, 6.46, 16.56, 22.03))
REDUCE_FROM = 7.8
SHARE_AT = (-1.71, 2.61, 4.03, 15.57, 17.98)


def layer_kernel(
    sp_count, tp_count, cuts,
    q_hbm, k_hbm, v_hbm, gate_hbm, decay_hbm, head_gain_hbm, w_out_hbm, ffn_gain_hbm,
    routing_hbm, weight_hbm, res_in_hbm, up_gate_hbm, up_hbm, down_hbm,
    out_ref,
    q_ref, k_ref, v_ref, gate_ref, decay_ref, head_gain_ref, ffn_gain_ref,
    routing_ref, weight_ref, res_ref,
    states, attended, opened, mixed, mixed_in, w_vmem,
    rows_all, share_all, gate_w, up_w, down_w, hidden, parts, got_core, got_one, got_two, got_mid, got_last, out_rows,
    in_sem, w_sem, state_send, state_recv, mix_send, mix_recv,
    share_send, share_recv, gather_send, gather_recv, swap_recv, reduce_send, reduce_recv, out_sem,
):
    sp_me, tp_me = lax.axis_index("sp"), lax.axis_index("tp")
    z_count = sp_count // 2
    z, x = sp_me // 2, lax.rem(sp_me, 2)
    y, c = tp_me // 2, lax.rem(tp_me, 2)
    barrier = pltpu.get_barrier_semaphore()

    @pl.loop(1, sp_count)
    def _(d):
        pl.semaphore_signal(
            barrier, inc=1, device_id={"sp": lax.rem(sp_me + d, sp_count)}, device_id_type=MESH
        )

    @pl.loop(1, tp_count)
    def _(d):
        pl.semaphore_signal(
            barrier, inc=1, device_id={"tp": lax.rem(tp_me + d, tp_count)}, device_id_type=MESH
        )

    small = [
        pltpu.make_async_copy(src, dst, in_sem.at[i])
        for i, (src, dst) in enumerate(
            (
                (decay_hbm, decay_ref), (k_hbm, k_ref), (v_hbm, v_ref), (q_hbm, q_ref),
                (routing_hbm, routing_ref), (weight_hbm, weight_ref), (gate_hbm, gate_ref),
                (head_gain_hbm, head_gain_ref), (ffn_gain_hbm, ffn_gain_ref), (res_in_hbm, res_ref),
            )
        )
    ]
    large = [
        pltpu.make_async_copy(src, dst, w_sem.at[i])
        for i, (src, dst) in enumerate(
            ((w_out_hbm, w_vmem), (up_gate_hbm, gate_w), (up_hbm, up_w), (down_hbm, down_w))
        )
    ]
    for load in small + large:
        load.start()

    def remote(src, dst, send, recv, target):
        return pltpu.make_async_remote_copy(
            src_ref=src, dst_ref=dst, send_sem=send, recv_sem=recv,
            device_id=target, device_id_type=MESH,
        )

    partner = {
        "x": {"sp": z * 2 + 1 - x},
        "y": {"tp": (1 - y) * 2 + c},
        "c": {"tp": y * 2 + 1 - c},
    }

    def z_peer(d):
        return {"sp": lax.rem(z + d, z_count) * 2 + x}

    tokens, key_lanes = q_ref.shape
    value_lanes = v_ref.shape[1]
    rows, width = res_ref.shape
    head_count = key_lanes // DK
    lane_head = lax.broadcasted_iota(jnp.int32, (1, key_lanes), 1) // DK
    small[0].wait()
    logit = decay_ref[...]
    log_decay = (jnp.minimum(logit, 0.0) - jnp.log1p(jnp.exp(-jnp.abs(logit)))) / DECAY_TEMP
    row_id = lax.broadcasted_iota(jnp.int32, (tokens, tokens), 0)
    col_id = lax.broadcasted_iota(jnp.int32, (tokens, tokens), 1)
    lower = jnp.where(row_id >= col_id, 1.0, 0.0).astype(jnp.bfloat16)
    top = log_decay.astype(jnp.bfloat16)
    rest = log_decay - top.astype(jnp.float32)
    middle = rest.astype(jnp.bfloat16)
    bottom = (rest - middle.astype(jnp.float32)).astype(jnp.bfloat16)
    sums = jnp.dot(
        lower,
        jnp.concatenate([top, middle, bottom], axis=1),
        preferred_element_type=jnp.float32,
    )
    cumulative = (
        sums[:, 2 * key_lanes :] + sums[:, key_lanes : 2 * key_lanes] + sums[:, :key_lanes]
    )
    for load in small[1:]:
        load.wait()
    keys = k_ref[...].astype(jnp.float32)
    query = q_ref[...].astype(jnp.float32) * DK ** (-0.5)
    values = v_ref[...]
    ending = cumulative[tokens - 1 :, :]
    wide = tn_dot(values, (keys * jnp.exp(ending - cumulative)).astype(jnp.bfloat16))
    state = jnp.zeros((DV, key_lanes), jnp.float32)
    for h in range(head_count):
        state = jnp.where(lane_head == h, wide[h * DV : (h + 1) * DV, :], state)
    passing = jnp.exp(ending)
    passing_hi = passing.astype(jnp.bfloat16).astype(jnp.float32)
    tail_row = lax.broadcasted_iota(jnp.int32, (16, key_lanes), 0)
    tail = jnp.where(
        tail_row == 0, passing_hi, jnp.where(tail_row == 1, passing - passing_hi, 0.0)
    )
    states[sp_me, 0:DV, :] = state.astype(jnp.bfloat16)
    states[sp_me, DV : DV + 16, :] = tail.astype(jnp.bfloat16)

    pl.semaphore_wait(barrier, sp_count + tp_count - 2)

    def state_copy(slot, d):
        return remote(
            states.at[slot], states.at[slot], state_send, state_recv,
            {"sp": lax.rem(sp_me + d, sp_count)},
        )

    @pl.loop(1, sp_count)
    def _(d):
        state_copy(sp_me, d).start()

    lane = lax.broadcasted_iota(jnp.int32, (LANES, tokens), 0)
    share = jnp.zeros((LANES, tokens), jnp.float32)
    spot = lax.broadcasted_iota(jnp.int32, (rows, tokens), 1)
    mine = spot == lax.broadcasted_iota(jnp.int32, (rows, tokens), 0) + tp_me * rows
    for j in range(weight_ref.shape[0]):
        weight = jnp.concatenate([weight_ref[j : j + 1, :]] * tp_count, axis=1)
        share = share + jnp.where(lane % (LANES // 2) == routing_ref[j : j + 1, :], weight, 0.0)
    share_hi = share.astype(jnp.bfloat16).astype(jnp.float32)
    share = jnp.where(lane < LANES // 2, share_hi, share - share_hi).astype(jnp.bfloat16)
    share_all[z, x, y, c] = nt_dot(mine.astype(jnp.bfloat16), share).astype(jnp.bfloat16)

    def spread(ref, lead, cols, order, stage, arriving, send, recv):
        at = {"z": z, "x": x, "y": y, "c": c}
        for axis in order[:stage]:
            at[axis] = slice(None)
        axis = order[stage]

        def block(place):
            return ref.at[(*lead, place["z"], place["x"], place["y"], place["c"], slice(None), cols)]

        if axis == "z" and arriving:
            src = block({**at, "z": slice(0, z_count - 1)})
            return [remote(src, src, send, recv, partner["x"])]
        src = block(at)
        if axis == "z":
            return [remote(src, src, send, recv, z_peer(d)) for d in range(1, z_count)]
        if arriving:
            src = block({**at, axis: 1 - at[axis]})
        return [remote(src, src, send, recv, partner[axis])]

    def share_copies(stage, arriving):
        return spread(
            share_all, (), slice(None), "zxyc", stage, arriving, share_send, share_recv.at[stage],
        )

    def share_step(stage):
        if stage:
            for copy in share_copies(stage - 1, True):
                copy.wait_recv()
        if stage < 4:
            for copy in share_copies(stage, False):
                copy.start()


    for i in range(tokens // SUB):
        first = i * SUB
        reach = min(-(-(first + SUB) // LANES) * LANES, tokens)
        start = cumulative[first - 1 : first, :] if i else jnp.zeros((1, key_lanes), jnp.float32)
        q_sub = query[first : first + SUB] * jnp.exp(cumulative[first : first + SUB] - start)
        k_sub = keys[:reach] * jnp.exp(jnp.minimum(start - cumulative[:reach], EXP_CAP))
        stacked = jnp.concatenate(
            [jnp.where(lane_head == h, q_sub, 0.0) for h in range(head_count)], axis=0
        )
        scores = nt_dot(stacked.astype(jnp.bfloat16), k_sub.astype(jnp.bfloat16))
        at_row = lax.broadcasted_iota(jnp.int32, scores.shape, 0) % SUB + first
        at_col = lax.broadcasted_iota(jnp.int32, scores.shape, 1)
        scores = jnp.where(at_row >= at_col, scores, 0.0).astype(jnp.bfloat16)
        inner = jnp.dot(scores, values[:reach], preferred_element_type=jnp.float32)
        for h in range(head_count):
            attended[first : first + SUB, h * DV : (h + 1) * DV] = inner[
                h * SUB : (h + 1) * SUB, h * DV : (h + 1) * DV
            ]
    for h in range(head_count):
        cols = slice(h * DV, (h + 1) * DV)
        wide_gate = gate_ref[:, cols].astype(jnp.float32)
        opened[:, cols] = (
            head_gain_ref[...].astype(jnp.float32) * wide_gate * jax.nn.sigmoid(wide_gate)
        )
    others = states.at[0 : sp_count - 1]
    state_all = remote(others, others, state_send, state_recv, partner["x"])
    state_all.wait_recv()

    def absorb(j, incoming):
        decay = states[j, DV : DV + 16, :].astype(jnp.float32)
        total = decay[0:1, :] + decay[1:2, :]
        return total * incoming + states[j, 0:DV, :].astype(jnp.float32)

    incoming = lax.fori_loop(
        0, sp_me, absorb, jnp.zeros((DV, key_lanes), jnp.float32)
    ).astype(jnp.bfloat16)
    query_dec = query * jnp.exp(cumulative)
    for h in range(head_count):
        cols = slice(h * DV, (h + 1) * DV)
        readout = nt_dot(jnp.where(lane_head == h, query_dec, 0.0).astype(jnp.bfloat16), incoming)
        head = attended[:, cols] + readout
        scale = lax.rsqrt(jnp.mean(head * head, axis=-1, keepdims=True) + NORM_EPS)
        mixed[:, cols] = (head * scale * opened[:, cols]).astype(jnp.bfloat16)

    def mix_copy(block, slot, d):
        return remote(
            mixed.at[pl.ds(pl.multiple_of(block * rows, rows), rows)], mixed_in.at[slot],
            mix_send, mix_recv, {"tp": lax.rem(tp_me + d, tp_count)},
        )

    for d in range(1, tp_count):
        mix_copy(lax.rem(tp_me + d, tp_count), tp_count - d - 1, d).start()
    large[0].wait()

    def w_rows(j):
        return w_vmem[pl.ds(pl.multiple_of(j * value_lanes, value_lanes), value_lanes), :]

    projected = jnp.dot(
        mixed[pl.ds(pl.multiple_of(tp_me * rows, rows), rows), :],
        w_rows(tp_me),
        preferred_element_type=jnp.float32,
    )
    incoming_mix = mixed_in.at[0 : tp_count - 1]
    mix_all = remote(incoming_mix, incoming_mix, mix_send, mix_recv, partner["c"])
    mix_all.wait_recv()
    for d in range(1, tp_count):
        slot = lax.rem(tp_me + d, tp_count)
        projected = projected + jnp.dot(
            mixed_in[d - 1], w_rows(slot), preferred_element_type=jnp.float32
        )
    residual = (res_ref[...].astype(jnp.float32) + projected).astype(jnp.bfloat16)
    res_ref[...] = residual
    wide_res = residual.astype(jnp.float32)
    inv = lax.rsqrt(jnp.mean(wide_res * wide_res, axis=-1, keepdims=True) + NORM_EPS)
    groups = rows // GROUP
    for k in range(width // LANES):
        cols = slice(k * LANES, (k + 1) * LANES)
        normed = wide_res[:, cols] * inv * ffn_gain_ref[k : k + 1, :].astype(jnp.float32)
        normed = normed.astype(jnp.bfloat16)
        for g in range(groups):
            rows_all[g, z, x, y, c, :, cols] = normed[g * GROUP : (g + 1) * GROUP]

    chunks = len(SPREAD)

    def span(q):
        return pl.ds(cuts[q][0], cuts[q][1])

    def gather_copies(g, q, stage, arriving):
        return spread(
            rows_all, (g,), span(q), SPREAD[q] + "c", stage, arriving,
            gather_send.at[g], gather_recv.at[g, q, stage] if stage < 3 else swap_recv.at[g],
        )

    def gather_step(g, q, stage):
        if stage:
            for copy in gather_copies(g, q, stage - 1, True):
                copy.wait_recv()
        for copy in gather_copies(g, q, stage, False):
            copy.start()

    def gathered(g):
        block = rows_all.at[g, :, :, :, 1 - c]
        remote(block, block, gather_send.at[g], swap_recv.at[g], partner["c"]).wait_recv()

    sent_blocks = sp_count * tp_count - 1

    def wait_sent(send, lanes):
        block = w_vmem.at[0 : sent_blocks * GROUP, 0:lanes]
        remote(block, block, send, share_recv.at[0], partner["c"]).wait_send()

    group_rows = sp_count * tp_count * GROUP
    half_rows = group_rows // 2
    half_z = z_count // 2

    def raise_half(g, half):
        zs = slice(half * half_z, (half + 1) * half_z)
        block = rows_all[g, zs].reshape(half_rows, width)
        gate_pre = jnp.dot(block, gate_w[...], preferred_element_type=jnp.float32)
        up_pre = jnp.dot(block, up_w[...], preferred_element_type=jnp.float32)
        tags = share_all[zs, :, :, :, pl.ds(pl.multiple_of(g * GROUP, GROUP), GROUP), :]
        tags = tags.reshape(half_rows, LANES).astype(jnp.float32)
        lane = lax.broadcasted_iota(jnp.int32, (half_rows, LANES), 1) % (LANES // 2)
        share = jnp.sum(jnp.where(lane == sp_me, tags, 0.0), axis=-1, keepdims=True)
        hidden[g, half * half_rows : (half + 1) * half_rows] = (
            clamped_unit(gate_pre, up_pre) * share
        ).astype(jnp.bfloat16)

    def lower_chunk(g, q):
        at, size = cuts[q]
        out = jnp.dot(hidden[g], down_w[:, at : at + size], preferred_element_type=jnp.float32)
        parts[g, :, :, :, :, :, at : at + size] = out.astype(jnp.bfloat16).reshape(
            z_count, 2, 2, 2, GROUP, size
        )

    every = slice(None)

    def reduce_order(q):
        return "c" + SPREAD[q][::-1]

    def reduce_copies(g, q, stage, arriving=False):
        order, cols = reduce_order(q), span(q)
        at = {"z": every, "x": every, "y": every, "c": every}
        for axis in order[:stage]:
            at[axis] = {"z": z, "x": x, "y": y, "c": c}[axis]
        axis = order[stage]

        def block(place):
            return parts.at[g, place["z"], place["x"], place["y"], place["c"], :, cols]

        send, recv = reduce_send.at[g], reduce_recv.at[g, q, stage]
        if axis == "z":
            dst = got_mid.at[g, :, :, :, cols] if stage == 2 else got_last.at[g, :, :, cols]
            if arriving:
                return [remote(dst, dst, send, recv, partner["x"])]
            return [
                remote(
                    block({**at, "z": lax.rem(z + d, z_count)}), dst.at[d - 1], send, recv, z_peer(d)
                )
                for d in range(1, z_count)
            ]
        own = {"x": x, "y": y, "c": c}[axis]
        dst = (
            got_core.at[g, :, :, :, :, cols] if stage == 0
            else got_one.at[g, :, :, :, cols] if stage == 1
            else got_two.at[g, :, :, cols] if stage == 2
            else got_last.at[g, 0, :, cols]
        )
        return [remote(block({**at, axis: 1 - own}), dst, send, recv, partner[axis])]

    def store(g, q):
        here = slice(g * GROUP, (g + 1) * GROUP)
        return pltpu.make_async_copy(
            out_rows.at[here, span(q)], out_ref.at[here, span(q)], out_sem
        )

    def f32(value):
        return value.astype(jnp.float32)

    def absorb_step(g, q, stage):
        for copy in reduce_copies(g, q, stage, True):
            copy.wait_recv()
        order = reduce_order(q)
        at, size = cuts[q]
        cols = slice(at, at + size)
        if stage == 0:
            @pl.loop(0, z_count)
            def _(zz):
                ours = parts[g, zz, :, :, c, :, cols]
                parts[g, zz, :, :, c, :, cols] = (
                    f32(ours) + f32(got_core[g, zz, :, :, :, cols])
                ).astype(jnp.bfloat16)
        elif stage == 1:
            where = (g, every, x, every, c) if order[1] == "x" else (g, every, every, y, c)
            where = (*where, every, cols)
            parts[where] = (f32(parts[where]) + f32(got_one[g, :, :, :, cols])).astype(jnp.bfloat16)
        elif stage == 2 and order[2] != "z":
            where = (g, every, x, y, c, every, cols)
            parts[where] = (f32(parts[where]) + f32(got_two[g, :, :, cols])).astype(jnp.bfloat16)
        elif stage == 2:
            where = (g, z, x, every, c) if order[1] == "x" else (g, z, every, y, c)
            where = (*where, every, cols)
            total = f32(parts[where])
            for d in range(1, z_count):
                total = total + f32(got_mid[g, d - 1, :, :, cols])
            parts[where] = total.astype(jnp.bfloat16)
        else:
            total = f32(parts[g, z, x, y, c, :, cols])
            for d in range(1, z_count if order[3] == "z" else 2):
                total = total + f32(got_last[g, d - 1, :, cols])
            here = slice(g * GROUP, (g + 1) * GROUP)
            out_rows[here, cols] = (f32(res_ref[here, cols]) + total).astype(jnp.bfloat16)
            store(g, q).start()

    def reduce_step(g, q, stage):
        if stage:
            absorb_step(g, q, stage - 1)
        if stage < 4:
            for copy in reduce_copies(g, q, stage):
                copy.start()

    events = []

    def plan(time, step, *args):
        events.append((time, len(events), step, args))

    def load_weights():
        for load in large[1:]:
            load.wait()

        state_all.wait_send()
        mix_all.wait_send()

    for i, time in enumerate(SHARE_AT):
        plan(time, share_step, i)
    for g in range(groups):
        ready = 0.0
        for q in range(chunks):
            for stage in range(4):
                plan(max(g * GATHER_PACE + GATHER_AT[q][stage], 0.0), gather_step, g, q, stage)
            ready = max(ready, g * GATHER_PACE + GATHER_AT[q][4])
        plan(ready, gathered, g)
        if g == 0:
            plan(ready, load_weights)
        plan(ready, raise_half, g, 0)
        plan(ready + RAISE_GAP, raise_half, g, 1)
        begin = max(ready + 2 * RAISE_GAP, REDUCE_FROM + g * REDUCE_PACE)
        for q in range(chunks):
            plan(begin + REDUCE_AT[q][0], lower_chunk, g, q)
            for stage in range(5):
                plan(begin + REDUCE_AT[q][stage], reduce_step, g, q, stage)
    for _, _, step, args in sorted(events, key=lambda event: event[:2]):
        step(*args)

    wait_sent(share_send, rows * LANES // GROUP)
    for g in range(groups):
        wait_sent(gather_send.at[g], width)
        wait_sent(reduce_send.at[g], width)
    pltpu.make_async_copy(out_rows, out_ref, out_sem).wait()


def column_cuts(width):
    tiles, total = width // LANES, sum(part for _, part in PIECES)
    cuts, passed = [], 0
    for _, part in PIECES:
        first, end = (tiles * n // total * LANES for n in (passed, passed + part))
        cuts.append((first, end - first))
        passed += part
    return cuts


def layer_rows(
    queries, key_rows, value_rows, out_gate, decay_logit, head_gain, w_out,
    ffn_gain, routing, route_weight, residual_in, gate_cols, up_cols, down_rows,
):
    sp_count, tp_count = lax.axis_size("sp"), lax.axis_size("tp")
    rows, width = residual_in.shape
    tokens, key_lanes = queries.shape
    value_lanes = value_rows.shape[1]
    units = gate_cols.shape[1]
    z_count, groups = sp_count // 2, rows // GROUP
    group_rows = sp_count * tp_count * GROUP
    cuts = column_cuts(width)
    hbm = pl.BlockSpec(memory_space=pl.ANY)
    bf16, f32 = jnp.bfloat16, jnp.float32
    dma = pltpu.SemaphoreType.DMA
    operands = (
        queries, key_rows, value_rows, out_gate, decay_logit, head_gain.reshape(1, -1), w_out,
        ffn_gain.reshape(-1, LANES), routing.T, route_weight.T, residual_in,
        gate_cols, up_cols, down_rows,
    )

    def like(array):
        return pltpu.VMEM(array.shape, array.dtype)

    return pl.pallas_call(
        functools.partial(layer_kernel, sp_count, tp_count, cuts),
        out_shape=jax.ShapeDtypeStruct((rows, width), bf16),
        in_specs=[hbm] * len(operands),
        out_specs=hbm,
        scratch_shapes=[
            *(like(operands[i]) for i in (0, 1, 2, 3, 4, 5, 7, 8, 9, 10)),
            pltpu.VMEM((sp_count, DV + 16, key_lanes), bf16),
            pltpu.VMEM((tokens, value_lanes), f32),
            pltpu.VMEM((tokens, value_lanes), f32),
            pltpu.VMEM((tokens, value_lanes), bf16),
            pltpu.VMEM((tp_count, rows, value_lanes), bf16),
            like(w_out),
            pltpu.VMEM((groups, z_count, 2, 2, 2, GROUP, width), bf16),
            pltpu.VMEM((z_count, 2, 2, 2, rows, LANES), bf16),
            like(gate_cols),
            like(up_cols),
            like(down_rows),
            pltpu.VMEM((groups, group_rows, units), bf16),
            pltpu.VMEM((groups, z_count, 2, 2, 2, GROUP, width), bf16),
            pltpu.VMEM((groups, z_count, 2, 2, GROUP, width), bf16),
            pltpu.VMEM((groups, z_count, 2, GROUP, width), bf16),
            pltpu.VMEM((groups, z_count, GROUP, width), bf16),
            pltpu.VMEM((groups, z_count - 1, 2, GROUP, width), bf16),
            pltpu.VMEM((groups, z_count - 1, GROUP, width), bf16),
            pltpu.VMEM((rows, width), bf16),
            dma((10,)),
            dma((4,)),
            dma,
            dma,
            dma,
            dma,
            dma,
            dma((4,)),
            dma((groups,)),
            dma((groups, len(cuts), 3)),
            dma((groups,)),
            dma((groups,)),
            dma((groups, len(cuts), 4)),
            dma,
        ],
        compiler_params=pltpu.CompilerParams(
            collective_id=1, has_side_effects=True, vmem_limit_bytes=62 << 20
        ),
        name="layer_rows",
    )(*operands)


def slot_ids(routes, capacity, experts):
    batch_size, rows_each, top_count = routes.shape
    flat_ids = routes.reshape(batch_size, rows_each * top_count)
    onehot = (flat_ids[:, :, None] == jnp.arange(experts, dtype=jnp.int32)[None, None, :]).astype(
        jnp.int32
    )
    earlier = jnp.cumsum(onehot, axis=1) - onehot
    rank_in = jnp.sum(earlier * onehot, axis=2)
    return (flat_ids * capacity + rank_in).reshape(batch_size, rows_each, top_count)


def dispatch_rows(slots, row_data, slot_total):
    chosen = jnp.any(slots[..., None] == jnp.arange(slot_total, dtype=jnp.int32), axis=2).astype(
        jnp.bfloat16
    )
    return jnp.einsum("brs,brd->bsd", chosen, row_data, preferred_element_type=jnp.float32).astype(
        jnp.bfloat16
    )


def on_device(
    residual_in,
    queries,
    key_rows,
    value_rows,
    out_gate,
    decay_logit,
    head_gain,
    w_out,
    ffn_gain,
    routing,
    route_weight,
    w_gate,
    w_up,
    w_down,
):
    tp_count = lax.axis_size("tp")
    experts = lax.axis_size("sp")
    quarter = residual_in.shape[0]
    top_count = routing.shape[1]
    model_width = residual_in.shape[1]
    capacity = 2 * routing.shape[0] * top_count // (tp_count * experts)
    slot_total = experts * capacity
    if (
        capacity >= quarter and experts <= LANES // 2 and experts % 4 == 0
        and tp_count == 4 and quarter % GROUP == 0
        and w_out.shape[0] >= (experts * tp_count - 1) * GROUP and model_width % (16 * LANES) == 0
        and quarter * LANES // GROUP <= model_width
    ):
        return layer_rows(
            queries, key_rows, value_rows, out_gate, decay_logit, head_gain, w_out,
            ffn_gain, routing, route_weight, residual_in, w_gate[0], w_up[0], w_down[0],
        )
    residual, extended = mix_rows(
        queries, key_rows, value_rows, out_gate, decay_logit, head_gain, w_out,
        ffn_gain, routing, route_weight, residual_in,
    )
    normed = extended[:, :model_width]
    gate_cols = w_gate[0]
    up_cols = w_up[0]
    down_rows = w_down[0]
    own_routes = lax.dynamic_slice_in_dim(routing, lax.axis_index("tp") * quarter, quarter, 0)
    own_slots = slot_ids(own_routes[None], capacity, experts)[0]
    outgoing = dispatch_rows(own_slots[None], normed[None], slot_total)[0]
    arrived = lax.all_to_all(
        outgoing.reshape(experts, capacity, model_width),
        "sp",
        split_axis=0,
        concat_axis=0,
        tiled=True,
    )
    portion = lax.all_gather(arrived[None], "tp", axis=0, tiled=True)
    flat_rows = portion.reshape(-1, model_width)
    gate_pre = jnp.dot(flat_rows, gate_cols, preferred_element_type=jnp.float32)
    up_pre = jnp.dot(flat_rows, up_cols, preferred_element_type=jnp.float32)
    hidden_rows = clamped_unit(gate_pre, up_pre).astype(jnp.bfloat16)
    hidden = hidden_rows.reshape(portion.shape[:-1] + (gate_cols.shape[1],))
    portion = hidden
    partial_out = jnp.dot(
        portion.reshape(-1, hidden.shape[-1]), down_rows, preferred_element_type=jnp.float32
    ).astype(jnp.bfloat16)
    partial_out = lax.optimization_barrier(partial_out)
    summed = lax.psum_scatter(
        partial_out.astype(jnp.float32)
        .reshape(portion.shape[:-1] + (model_width,))
        .astype(jnp.bfloat16),
        "tp",
        scatter_dimension=0,
        tiled=True,
    ).astype(jnp.float32)
    returned = lax.all_to_all(
        summed[0].astype(jnp.bfloat16), "sp", split_axis=0, concat_axis=0, tiled=True
    )
    picked = jnp.take(
        returned.reshape(slot_total, model_width), own_slots.reshape(-1), axis=0
    ).reshape(quarter, top_count, model_width)
    routed = jnp.sum(picked.astype(jnp.float32) * route_weight[:, :, None], axis=1)
    return (residual.astype(jnp.float32) + routed).astype(jnp.bfloat16)


def solution(mesh):
    placed = (
        P(("sp", "tp"), None),
        P("sp", "tp"),
        P("sp", "tp"),
        P("sp", "tp"),
        P("sp", "tp"),
        P("sp", "tp"),
        P(),
        P(),
        P(),
        P("sp", None),
        P(("sp", "tp"), None),
        P("sp", None, "tp"),
        P("sp", None, "tp"),
        P("sp", "tp", None),
    )
    return jax.shard_map(
        on_device, mesh=mesh, in_specs=placed, out_specs=P(("sp", "tp"), None), check_vma=False
    )
```

```python
import jax
import jax.numpy as jnp
from jax import lax
from jax.experimental import pallas as pl
from jax.experimental.pallas import tpu as pltpu
from jax.sharding import PartitionSpec as P
import functools

DK = 64
DV = 128


DECAY_TEMP = 16.0
CLAMP_LIMIT = 7.0
SIGMOID_SLOPE = 1.702
NORM_EPS = 1e-06
EXACT_PRECISION = lax.Precision.HIGHEST


def clamped_unit(gate_pre, up_pre):
    gate_cut = jnp.minimum(gate_pre, CLAMP_LIMIT)
    up_cut = jnp.clip(up_pre, -CLAMP_LIMIT, CLAMP_LIMIT)
    return (up_cut + 1.0) * (gate_cut * jax.nn.sigmoid(SIGMOID_SLOPE * gate_cut))


MESH = pl.DeviceIdType.MESH
LANES = 128
SUB = 32
EXP_CAP = 64.0


def nt_dot(left, right):
    return lax.dot_general(
        left, right, (((1,), (1,)), ((), ())), preferred_element_type=jnp.float32
    )


def tn_dot(left, right):
    return lax.dot_general(
        left, right, (((0,), (0,)), ((), ())), preferred_element_type=jnp.float32
    )


def mix_kernel(
    sp_count, tp_count,
    q_ref, k_ref, v_ref, gate_ref, decay_ref, head_gain_ref, w_hbm, ffn_gain_ref,
    routing_ref, weight_ref, res_in_ref,
    res_ref, ext_ref,
    states, attended, mixed, mixed_in, w_vmem,
    w_sem, state_send, state_recv, mix_send, mix_recv,
):
    sp_me, tp_me = lax.axis_index("sp"), lax.axis_index("tp")
    barrier = pltpu.get_barrier_semaphore()

    @pl.loop(1, sp_count)
    def _(d):
        pl.semaphore_signal(
            barrier, inc=1, device_id={"sp": lax.rem(sp_me + d, sp_count)}, device_id_type=MESH
        )

    @pl.loop(1, tp_count)
    def _(d):
        pl.semaphore_signal(
            barrier, inc=1, device_id={"tp": lax.rem(tp_me + d, tp_count)}, device_id_type=MESH
        )

    w_copy = pltpu.make_async_copy(w_hbm, w_vmem, w_sem)
    w_copy.start()

    tokens, key_lanes = q_ref.shape
    value_lanes = v_ref.shape[1]
    head_count = key_lanes // DK
    lane_head = lax.broadcasted_iota(jnp.int32, (1, key_lanes), 1) // DK
    logit = decay_ref[...]
    log_decay = (jnp.minimum(logit, 0.0) - jnp.log1p(jnp.exp(-jnp.abs(logit)))) / DECAY_TEMP
    row_id = lax.broadcasted_iota(jnp.int32, (tokens, tokens), 0)
    col_id = lax.broadcasted_iota(jnp.int32, (tokens, tokens), 1)
    lower = (row_id >= col_id).astype(jnp.float32)
    cumulative = jnp.dot(
        lower, log_decay, precision=EXACT_PRECISION, preferred_element_type=jnp.float32
    )
    keys = k_ref[...].astype(jnp.float32)
    query = q_ref[...].astype(jnp.float32) * DK ** (-0.5)
    values = v_ref[...]
    ending = cumulative[tokens - 1 :, :]
    wide = tn_dot(values, (keys * jnp.exp(ending - cumulative)).astype(jnp.bfloat16))
    state = jnp.zeros((DV, key_lanes), jnp.float32)
    for h in range(head_count):
        state = jnp.where(lane_head == h, wide[h * DV : (h + 1) * DV, :], state)
    passing = jnp.exp(ending)
    passing_hi = passing.astype(jnp.bfloat16).astype(jnp.float32)
    tail_row = lax.broadcasted_iota(jnp.int32, (16, key_lanes), 0)
    tail = jnp.where(
        tail_row == 0, passing_hi, jnp.where(tail_row == 1, passing - passing_hi, 0.0)
    )
    states[sp_me, 0:DV, :] = state.astype(jnp.bfloat16)
    states[sp_me, DV : DV + 16, :] = tail.astype(jnp.bfloat16)

    pl.semaphore_wait(barrier, sp_count + tp_count - 2)

    def state_copy(slot, d):
        return pltpu.make_async_remote_copy(
            src_ref=states.at[slot],
            dst_ref=states.at[slot],
            send_sem=state_send.at[d],
            recv_sem=state_recv.at[slot],
            device_id={"sp": lax.rem(sp_me + d, sp_count)},
            device_id_type=MESH,
        )

    @pl.loop(1, sp_count)
    def _(d):
        state_copy(sp_me, d).start()

    for i in range(tokens // SUB):
        first = i * SUB
        reach = min(-(-(first + SUB) // LANES) * LANES, tokens)
        start = cumulative[first - 1 : first, :] if i else jnp.zeros((1, key_lanes), jnp.float32)
        q_sub = query[first : first + SUB] * jnp.exp(cumulative[first : first + SUB] - start)
        k_sub = keys[:reach] * jnp.exp(jnp.minimum(start - cumulative[:reach], EXP_CAP))
        stacked = jnp.concatenate(
            [jnp.where(lane_head == h, q_sub, 0.0) for h in range(head_count)], axis=0
        )
        scores = nt_dot(stacked.astype(jnp.bfloat16), k_sub.astype(jnp.bfloat16))
        at_row = lax.broadcasted_iota(jnp.int32, scores.shape, 0) % SUB + first
        at_col = lax.broadcasted_iota(jnp.int32, scores.shape, 1)
        scores = jnp.where(at_row >= at_col, scores, 0.0).astype(jnp.bfloat16)
        inner = jnp.dot(scores, values[:reach], preferred_element_type=jnp.float32)
        for h in range(head_count):
            attended[first : first + SUB, h * DV : (h + 1) * DV] = inner[
                h * SUB : (h + 1) * SUB, h * DV : (h + 1) * DV
            ]

    @pl.loop(1, sp_count)
    def _(d):
        state_copy(lax.rem(sp_me + d, sp_count), d).wait_recv()

    def absorb(j, incoming):
        decay = states[j, DV : DV + 16, :].astype(jnp.float32)
        total = decay[0:1, :] + decay[1:2, :]
        following = total * incoming + states[j, 0:DV, :].astype(jnp.float32)
        return jnp.where(j < sp_me, following, incoming)

    incoming = lax.fori_loop(
        0, sp_count, absorb, jnp.zeros((DV, key_lanes), jnp.float32)
    ).astype(jnp.bfloat16)
    query_dec = query * jnp.exp(cumulative)
    for h in range(head_count):
        cols = slice(h * DV, (h + 1) * DV)
        readout = nt_dot(jnp.where(lane_head == h, query_dec, 0.0).astype(jnp.bfloat16), incoming)
        head = attended[:, cols] + readout
        scale = lax.rsqrt(jnp.mean(head * head, axis=-1, keepdims=True) + NORM_EPS)
        opened = gate_ref[:, cols].astype(jnp.float32)
        opened = opened * jax.nn.sigmoid(opened)
        mixed[:, cols] = (head * scale * head_gain_ref[...].astype(jnp.float32) * opened).astype(
            jnp.bfloat16
        )

    rows = res_in_ref.shape[0]

    def mix_copy(block, slot, d):
        return pltpu.make_async_remote_copy(
            src_ref=mixed.at[pl.ds(pl.multiple_of(block * rows, rows), rows)],
            dst_ref=mixed_in.at[slot],
            send_sem=mix_send.at[d],
            recv_sem=mix_recv.at[slot],
            device_id={"tp": lax.rem(tp_me + d, tp_count)},
            device_id_type=MESH,
        )

    for d in range(1, tp_count):
        mix_copy(lax.rem(tp_me + d, tp_count), tp_me, d).start()

    lane = lax.broadcasted_iota(jnp.int32, (rows, LANES), 1)
    named = routing_ref[pl.ds(pl.multiple_of(tp_me * rows, rows), rows), :]
    share = jnp.zeros((rows, LANES), jnp.float32)
    for j in range(weight_ref.shape[1]):
        share = share + jnp.where(
            lane % (LANES // 2) == named[:, j : j + 1], weight_ref[:, j : j + 1], 0.0
        )
    share_hi = share.astype(jnp.bfloat16).astype(jnp.float32)
    width = res_in_ref.shape[1]
    ext_ref[:, width:] = jnp.where(lane < LANES // 2, share_hi, share - share_hi).astype(
        jnp.bfloat16
    )

    w_copy.wait()

    def w_rows(j):
        return w_vmem[pl.ds(pl.multiple_of(j * value_lanes, value_lanes), value_lanes), :]

    projected = jnp.dot(
        mixed[pl.ds(pl.multiple_of(tp_me * rows, rows), rows), :],
        w_rows(tp_me),
        preferred_element_type=jnp.float32,
    )
    for d in range(1, tp_count):
        slot = lax.rem(tp_me + d, tp_count)
        mix_copy(slot, slot, d).wait_recv()
        projected = projected + jnp.dot(
            mixed_in[slot], w_rows(slot), preferred_element_type=jnp.float32
        )
    residual = (res_in_ref[...].astype(jnp.float32) + projected).astype(jnp.bfloat16)
    res_ref[...] = residual
    wide_res = residual.astype(jnp.float32)
    inv = lax.rsqrt(jnp.mean(wide_res * wide_res, axis=-1, keepdims=True) + NORM_EPS)
    ext_ref[:, :width] = (wide_res * inv * ffn_gain_ref[...].astype(jnp.float32)).astype(
        jnp.bfloat16
    )

    @pl.loop(1, sp_count)
    def _(d):
        state_copy(sp_me, d).wait_send()

    for d in range(1, tp_count):
        mix_copy(lax.rem(tp_me + d, tp_count), tp_me, d).wait_send()


def mix_rows(
    queries, key_rows, value_rows, out_gate, decay_logit, head_gain, w_out,
    ffn_gain, routing, route_weight, residual_in,
):
    sp_count, tp_count = lax.axis_size("sp"), lax.axis_size("tp")
    rows, width = residual_in.shape
    tokens, key_lanes = queries.shape
    value_lanes = value_rows.shape[1]
    vmem = pl.BlockSpec(memory_space=pltpu.VMEM)
    return pl.pallas_call(
        functools.partial(mix_kernel, sp_count, tp_count),
        out_shape=(
            jax.ShapeDtypeStruct((rows, width), jnp.bfloat16),
            jax.ShapeDtypeStruct((rows, width + LANES), jnp.bfloat16),
        ),
        in_specs=[vmem] * 6 + [pl.BlockSpec(memory_space=pl.ANY)] + [vmem] * 4,
        out_specs=(vmem, vmem),
        scratch_shapes=[
            pltpu.VMEM((sp_count, DV + 16, key_lanes), jnp.bfloat16),
            pltpu.VMEM((tokens, value_lanes), jnp.float32),
            pltpu.VMEM((tokens, value_lanes), jnp.bfloat16),
            pltpu.VMEM((tp_count, rows, value_lanes), jnp.bfloat16),
            pltpu.VMEM(w_out.shape, jnp.bfloat16),
            pltpu.SemaphoreType.DMA,
            pltpu.SemaphoreType.DMA((sp_count,)),
            pltpu.SemaphoreType.DMA((sp_count,)),
            pltpu.SemaphoreType.DMA((tp_count,)),
            pltpu.SemaphoreType.DMA((tp_count,)),
        ],
        compiler_params=pltpu.CompilerParams(
            collective_id=0, has_side_effects=True, vmem_limit_bytes=40 << 20
        ),
        name="mix_rows",
    )(
        queries, key_rows, value_rows, out_gate, decay_logit, head_gain.reshape(1, -1), w_out,
        ffn_gain.reshape(1, -1), routing, route_weight, residual_in,
    )


GROUP = 16
PIECES = (('zxy', 5), ('zyx', 5), ('xzy', 3), ('yzx', 3))
SPREAD = tuple(order for order, _ in PIECES)
GATHER_PACE, REDUCE_PACE, RAISE_GAP = 5.93, 0.99, 0.74
GATHER_AT = ((-0.39, 3.6, 7.61, 22.71, 27.52), (-0.09, 7.59, 11.49, 18.04, 27.81), (-10.56, 9.95, 16.61, 26.65, 28.74), (-4.53, 8.4, 15.26, 20.77, 24.71))
REDUCE_AT = ((0.0, 1.36, 6.01, 10.78, 26.83), (0.43, 4.07, 10.15, 15.03, 38.01), (0.86, 3.15, 8.38, 17.57, 24.05), (1.29, 3.51, 6.46, 16.56, 22.03))
REDUCE_FROM = 7.8
SHARE_AT = (-1.71, 2.61, 4.03, 15.57, 17.98)


def layer_kernel(
    sp_count, tp_count, cuts,
    q_hbm, k_hbm, v_hbm, gate_hbm, decay_hbm, head_gain_hbm, w_out_hbm, ffn_gain_hbm,
    routing_hbm, weight_hbm, res_in_hbm, up_gate_hbm, up_hbm, down_hbm,
    out_ref,
    q_ref, k_ref, v_ref, gate_ref, decay_ref, head_gain_ref, ffn_gain_ref,
    routing_ref, weight_ref, res_ref,
    states, passed, attended, opened, mixed, mixed_in, w_vmem,
    rows_all, share_all, gate_w, up_w, down_w, hidden, parts, got_core, got_one, got_two, got_mid, got_last, out_rows,
    in_sem, w_sem, state_send, state_recv, passed_send, passed_recv, mix_send, mix_recv,
    share_send, share_recv, gather_send, gather_recv, swap_recv, reduce_send, reduce_recv, out_sem,
):
    sp_me, tp_me = lax.axis_index("sp"), lax.axis_index("tp")
    z_count = sp_count // 2
    z, x = sp_me // 2, lax.rem(sp_me, 2)
    y, c = tp_me // 2, lax.rem(tp_me, 2)
    barrier = pltpu.get_barrier_semaphore()

    @pl.loop(1, sp_count)
    def _(d):
        pl.semaphore_signal(
            barrier, inc=1, device_id={"sp": lax.rem(sp_me + d, sp_count)}, device_id_type=MESH
        )

    @pl.loop(1, tp_count)
    def _(d):
        pl.semaphore_signal(
            barrier, inc=1, device_id={"tp": lax.rem(tp_me + d, tp_count)}, device_id_type=MESH
        )

    small = [
        pltpu.make_async_copy(src, dst, in_sem.at[i])
        for i, (src, dst) in enumerate(
            (
                (decay_hbm, decay_ref), (k_hbm, k_ref), (v_hbm, v_ref), (q_hbm, q_ref),
                (routing_hbm, routing_ref), (weight_hbm, weight_ref), (gate_hbm, gate_ref),
                (head_gain_hbm, head_gain_ref), (ffn_gain_hbm, ffn_gain_ref), (res_in_hbm, res_ref),
            )
        )
    ]
    large = [
        pltpu.make_async_copy(src, dst, w_sem.at[i])
        for i, (src, dst) in enumerate(
            ((w_out_hbm, w_vmem), (up_gate_hbm, gate_w), (up_hbm, up_w), (down_hbm, down_w))
        )
    ]
    for load in small + large:
        load.start()

    def remote(src, dst, send, recv, target):
        return pltpu.make_async_remote_copy(
            src_ref=src, dst_ref=dst, send_sem=send, recv_sem=recv,
            device_id=target, device_id_type=MESH,
        )

    partner = {
        "x": {"sp": z * 2 + 1 - x},
        "y": {"tp": (1 - y) * 2 + c},
        "c": {"tp": y * 2 + 1 - c},
    }

    def z_peer(d):
        return {"sp": lax.rem(z + d, z_count) * 2 + x}

    tokens, key_lanes = q_ref.shape
    value_lanes = v_ref.shape[1]
    rows, width = res_ref.shape
    head_count = key_lanes // DK
    lane_head = lax.broadcasted_iota(jnp.int32, (1, key_lanes), 1) // DK
    small[0].wait()
    logit = decay_ref[...]
    log_decay = (jnp.minimum(logit, 0.0) - jnp.log1p(jnp.exp(-jnp.abs(logit)))) / DECAY_TEMP
    row_id = lax.broadcasted_iota(jnp.int32, (tokens, tokens), 0)
    col_id = lax.broadcasted_iota(jnp.int32, (tokens, tokens), 1)
    lower = jnp.where(row_id >= col_id, 1.0, 0.0).astype(jnp.bfloat16)
    top = log_decay.astype(jnp.bfloat16)
    rest = log_decay - top.astype(jnp.float32)
    middle = rest.astype(jnp.bfloat16)
    bottom = (rest - middle.astype(jnp.float32)).astype(jnp.bfloat16)
    sums = jnp.dot(
        lower,
        jnp.concatenate([top, middle, bottom], axis=1),
        preferred_element_type=jnp.float32,
    )
    cumulative = (
        sums[:, 2 * key_lanes :] + sums[:, key_lanes : 2 * key_lanes] + sums[:, :key_lanes]
    )
    for load in small[1:]:
        load.wait()
    keys = k_ref[...].astype(jnp.float32)
    query = q_ref[...].astype(jnp.float32) * DK ** (-0.5)
    values = v_ref[...]
    ending = cumulative[tokens - 1 :, :]
    wide = tn_dot(values, (keys * jnp.exp(ending - cumulative)).astype(jnp.bfloat16))
    state = jnp.zeros((DV, key_lanes), jnp.float32)
    for h in range(head_count):
        state = jnp.where(lane_head == h, wide[h * DV : (h + 1) * DV, :], state)
    states[sp_me] = state.astype(jnp.bfloat16)
    passed[sp_me] = jnp.exp(ending)

    pl.semaphore_wait(barrier, sp_count + tp_count - 2)

    def state_copy(slot, d):
        return remote(
            states.at[slot], states.at[slot], state_send, state_recv,
            {"sp": lax.rem(sp_me + d, sp_count)},
        )

    def passed_copy(slot, d):
        return remote(
            passed.at[slot], passed.at[slot], passed_send, passed_recv,
            {"sp": lax.rem(sp_me + d, sp_count)},
        )

    @pl.loop(1, sp_count)
    def _(d):
        passed_copy(sp_me, d).start()
        state_copy(sp_me, d).start()

    lane = lax.broadcasted_iota(jnp.int32, (LANES, tokens), 0)
    share = jnp.zeros((LANES, tokens), jnp.float32)
    spot = lax.broadcasted_iota(jnp.int32, (rows, tokens), 1)
    mine = spot == lax.broadcasted_iota(jnp.int32, (rows, tokens), 0) + tp_me * rows
    for j in range(weight_ref.shape[0]):
        weight = jnp.concatenate([weight_ref[j : j + 1, :]] * tp_count, axis=1)
        share = share + jnp.where(lane % (LANES // 2) == routing_ref[j : j + 1, :], weight, 0.0)
    share_hi = share.astype(jnp.bfloat16).astype(jnp.float32)
    share = jnp.where(lane < LANES // 2, share_hi, share - share_hi).astype(jnp.bfloat16)
    share_all[z, x, y, c] = nt_dot(mine.astype(jnp.bfloat16), share).astype(jnp.bfloat16)

    def spread(ref, lead, cols, order, stage, arriving, send, recv):
        at = {"z": z, "x": x, "y": y, "c": c}
        for axis in order[:stage]:
            at[axis] = slice(None)
        axis = order[stage]

        def block(place):
            return ref.at[(*lead, place["z"], place["x"], place["y"], place["c"], slice(None), cols)]

        if axis == "z" and arriving:
            src = block({**at, "z": slice(0, z_count - 1)})
            return [remote(src, src, send, recv, partner["x"])]
        src = block(at)
        if axis == "z":
            return [remote(src, src, send, recv, z_peer(d)) for d in range(1, z_count)]
        if arriving:
            src = block({**at, axis: 1 - at[axis]})
        return [remote(src, src, send, recv, partner[axis])]

    def share_copies(stage, arriving):
        return spread(
            share_all, (), slice(None), "zxyc", stage, arriving, share_send, share_recv.at[stage],
        )

    def share_step(stage):
        if stage:
            for copy in share_copies(stage - 1, True):
                copy.wait_recv()
        if stage < 4:
            for copy in share_copies(stage, False):
                copy.start()


    for i in range(tokens // SUB):
        first = i * SUB
        reach = min(-(-(first + SUB) // LANES) * LANES, tokens)
        start = cumulative[first - 1 : first, :] if i else jnp.zeros((1, key_lanes), jnp.float32)
        q_sub = query[first : first + SUB] * jnp.exp(cumulative[first : first + SUB] - start)
        k_sub = keys[:reach] * jnp.exp(jnp.minimum(start - cumulative[:reach], EXP_CAP))
        stacked = jnp.concatenate(
            [jnp.where(lane_head == h, q_sub, 0.0) for h in range(head_count)], axis=0
        )
        scores = nt_dot(stacked.astype(jnp.bfloat16), k_sub.astype(jnp.bfloat16))
        at_row = lax.broadcasted_iota(jnp.int32, scores.shape, 0) % SUB + first
        at_col = lax.broadcasted_iota(jnp.int32, scores.shape, 1)
        scores = jnp.where(at_row >= at_col, scores, 0.0).astype(jnp.bfloat16)
        inner = jnp.dot(scores, values[:reach], preferred_element_type=jnp.float32)
        for h in range(head_count):
            attended[first : first + SUB, h * DV : (h + 1) * DV] = inner[
                h * SUB : (h + 1) * SUB, h * DV : (h + 1) * DV
            ]
    for h in range(head_count):
        cols = slice(h * DV, (h + 1) * DV)
        wide_gate = gate_ref[:, cols].astype(jnp.float32)
        opened[:, cols] = (
            head_gain_ref[...].astype(jnp.float32) * wide_gate * jax.nn.sigmoid(wide_gate)
        )
    others = states.at[0 : sp_count - 1]
    state_all = remote(others, others, state_send, state_recv, partner["x"])
    state_all.wait_recv()
    others = passed.at[0 : sp_count - 1]
    passed_all = remote(others, others, passed_send, passed_recv, partner["x"])
    passed_all.wait_recv()

    def absorb(j, incoming):
        return passed[j] * incoming + states[j].astype(jnp.float32)

    incoming = lax.fori_loop(
        0, sp_me, absorb, jnp.zeros((DV, key_lanes), jnp.float32)
    ).astype(jnp.bfloat16)
    query_dec = query * jnp.exp(cumulative)
    for h in range(head_count):
        cols = slice(h * DV, (h + 1) * DV)
        readout = nt_dot(jnp.where(lane_head == h, query_dec, 0.0).astype(jnp.bfloat16), incoming)
        head = attended[:, cols] + readout
        scale = lax.rsqrt(jnp.mean(head * head, axis=-1, keepdims=True) + NORM_EPS)
        mixed[:, cols] = (head * scale * opened[:, cols]).astype(jnp.bfloat16)

    def mix_copy(block, i):
        return remote(
            mixed.at[pl.ds(pl.multiple_of(block * rows, rows), rows)], mixed_in.at[i],
            mix_send, mix_recv.at[i], {"tp": block},
        )

    others = ((y, 1 - c), (1 - y, c), (1 - y, 1 - c))
    for i, (yy, cc) in enumerate(others):
        mix_copy(yy * 2 + cc, i).start()
    large[0].wait()

    def w_rows(j):
        return w_vmem[pl.ds(pl.multiple_of(j * value_lanes, value_lanes), value_lanes), :]

    projected = jnp.dot(
        mixed[pl.ds(pl.multiple_of(tp_me * rows, rows), rows), :],
        w_rows(tp_me),
        preferred_element_type=jnp.float32,
    )
    for i, (yy, cc) in enumerate(others):
        mix_copy(yy * 2 + cc, i).wait_recv()
        projected = projected + jnp.dot(
            mixed_in[i], w_rows(yy * 2 + cc), preferred_element_type=jnp.float32
        )
    mix_all = remote(mixed_in, mixed_in, mix_send, mix_recv.at[0], partner["c"])
    residual = (res_ref[...].astype(jnp.float32) + projected).astype(jnp.bfloat16)
    res_ref[...] = residual
    wide_res = residual.astype(jnp.float32)
    inv = lax.rsqrt(jnp.mean(wide_res * wide_res, axis=-1, keepdims=True) + NORM_EPS)
    groups = rows // GROUP
    for k in range(width // LANES):
        cols = slice(k * LANES, (k + 1) * LANES)
        normed = wide_res[:, cols] * inv * ffn_gain_ref[k : k + 1, :].astype(jnp.float32)
        normed = normed.astype(jnp.bfloat16)
        for g in range(groups):
            rows_all[g, z, x, y, c, :, cols] = normed[g * GROUP : (g + 1) * GROUP]

    chunks = len(SPREAD)

    def span(q):
        return pl.ds(cuts[q][0], cuts[q][1])

    def gather_copies(g, q, stage, arriving):
        return spread(
            rows_all, (g,), span(q), SPREAD[q] + "c", stage, arriving,
            gather_send.at[g], gather_recv.at[g, q, stage] if stage < 3 else swap_recv.at[g],
        )

    def gather_step(g, q, stage):
        if stage:
            for copy in gather_copies(g, q, stage - 1, True):
                copy.wait_recv()
        for copy in gather_copies(g, q, stage, False):
            copy.start()

    def gathered(g):
        block = rows_all.at[g, :, :, :, 1 - c]
        remote(block, block, gather_send.at[g], swap_recv.at[g], partner["c"]).wait_recv()

    sent_blocks = sp_count * tp_count - 1

    def wait_sent(send, lanes):
        block = w_vmem.at[0 : sent_blocks * GROUP, 0:lanes]
        remote(block, block, send, share_recv.at[0], partner["c"]).wait_send()

    group_rows = sp_count * tp_count * GROUP
    half_rows = group_rows // 2
    half_z = z_count // 2

    def raise_half(g, half):
        zs = slice(half * half_z, (half + 1) * half_z)
        block = rows_all[g, zs].reshape(half_rows, width)
        gate_pre = jnp.dot(block, gate_w[...], preferred_element_type=jnp.float32)
        up_pre = jnp.dot(block, up_w[...], preferred_element_type=jnp.float32)
        tags = share_all[zs, :, :, :, pl.ds(pl.multiple_of(g * GROUP, GROUP), GROUP), :]
        tags = tags.reshape(half_rows, LANES).astype(jnp.float32)
        lane = lax.broadcasted_iota(jnp.int32, (half_rows, LANES), 1) % (LANES // 2)
        share = jnp.sum(jnp.where(lane == sp_me, tags, 0.0), axis=-1, keepdims=True)
        hidden[g, half * half_rows : (half + 1) * half_rows] = (
            clamped_unit(gate_pre, up_pre) * share
        ).astype(jnp.bfloat16)

    def lower_chunk(g, q):
        at, size = cuts[q]
        out = jnp.dot(hidden[g], down_w[:, at : at + size], preferred_element_type=jnp.float32)
        parts[g, :, :, :, :, :, at : at + size] = out.astype(jnp.bfloat16).reshape(
            z_count, 2, 2, 2, GROUP, size
        )

    every = slice(None)

    def reduce_order(q):
        return "c" + SPREAD[q][::-1]

    def reduce_copies(g, q, stage, arriving=False):
        order, cols = reduce_order(q), span(q)
        at = {"z": every, "x": every, "y": every, "c": every}
        for axis in order[:stage]:
            at[axis] = {"z": z, "x": x, "y": y, "c": c}[axis]
        axis = order[stage]

        def block(place):
            return parts.at[g, place["z"], place["x"], place["y"], place["c"], :, cols]

        send, recv = reduce_send.at[g], reduce_recv.at[g, q, stage]
        if axis == "z":
            dst = got_mid.at[g, :, :, :, cols] if stage == 2 else got_last.at[g, :, :, cols]
            if arriving:
                return [remote(dst, dst, send, recv, partner["x"])]
            return [
                remote(
                    block({**at, "z": lax.rem(z + d, z_count)}), dst.at[d - 1], send, recv, z_peer(d)
                )
                for d in range(1, z_count)
            ]
        own = {"x": x, "y": y, "c": c}[axis]
        dst = (
            got_core.at[g, :, :, :, :, cols] if stage == 0
            else got_one.at[g, :, :, :, cols] if stage == 1
            else got_two.at[g, :, :, cols] if stage == 2
            else got_last.at[g, 0, :, cols]
        )
        return [remote(block({**at, axis: 1 - own}), dst, send, recv, partner[axis])]

    def store(g, q):
        here = slice(g * GROUP, (g + 1) * GROUP)
        return pltpu.make_async_copy(
            out_rows.at[here, span(q)], out_ref.at[here, span(q)], out_sem
        )

    def f32(value):
        return value.astype(jnp.float32)

    def absorb_step(g, q, stage):
        for copy in reduce_copies(g, q, stage, True):
            copy.wait_recv()
        order = reduce_order(q)
        at, size = cuts[q]
        cols = slice(at, at + size)
        if stage == 0:
            @pl.loop(0, z_count)
            def _(zz):
                ours = parts[g, zz, :, :, c, :, cols]
                parts[g, zz, :, :, c, :, cols] = (
                    f32(ours) + f32(got_core[g, zz, :, :, :, cols])
                ).astype(jnp.bfloat16)
        elif stage == 1:
            where = (g, every, x, every, c) if order[1] == "x" else (g, every, every, y, c)
            where = (*where, every, cols)
            parts[where] = (f32(parts[where]) + f32(got_one[g, :, :, :, cols])).astype(jnp.bfloat16)
        elif stage == 2 and order[2] != "z":
            where = (g, every, x, y, c, every, cols)
            parts[where] = (f32(parts[where]) + f32(got_two[g, :, :, cols])).astype(jnp.bfloat16)
        elif stage == 2:
            where = (g, z, x, every, c) if order[1] == "x" else (g, z, every, y, c)
            where = (*where, every, cols)
            total = f32(parts[where])
            for d in range(1, z_count):
                total = total + f32(got_mid[g, d - 1, :, :, cols])
            parts[where] = total.astype(jnp.bfloat16)
        else:
            total = f32(parts[g, z, x, y, c, :, cols])
            for d in range(1, z_count if order[3] == "z" else 2):
                total = total + f32(got_last[g, d - 1, :, cols])
            here = slice(g * GROUP, (g + 1) * GROUP)
            out_rows[here, cols] = (f32(res_ref[here, cols]) + total).astype(jnp.bfloat16)
            store(g, q).start()

    def reduce_step(g, q, stage):
        if stage:
            absorb_step(g, q, stage - 1)
        if stage < 4:
            for copy in reduce_copies(g, q, stage):
                copy.start()

    events = []

    def plan(time, step, *args):
        events.append((time, len(events), step, args))

    def load_weights():
        for load in large[1:]:
            load.wait()

        state_all.wait_send()
        passed_all.wait_send()
        mix_all.wait_send()

    for i, time in enumerate(SHARE_AT):
        plan(time, share_step, i)
    for g in range(groups):
        ready = 0.0
        for q in range(chunks):
            for stage in range(4):
                plan(max(g * GATHER_PACE + GATHER_AT[q][stage], 0.0), gather_step, g, q, stage)
            ready = max(ready, g * GATHER_PACE + GATHER_AT[q][4])
        plan(ready, gathered, g)
        if g == 0:
            plan(ready, load_weights)
        plan(ready, raise_half, g, 0)
        plan(ready + RAISE_GAP, raise_half, g, 1)
        begin = max(ready + 2 * RAISE_GAP, REDUCE_FROM + g * REDUCE_PACE)
        for q in range(chunks):
            plan(begin + REDUCE_AT[q][0], lower_chunk, g, q)
            for stage in range(5):
                plan(begin + REDUCE_AT[q][stage], reduce_step, g, q, stage)
    for _, _, step, args in sorted(events, key=lambda event: event[:2]):
        step(*args)

    wait_sent(share_send, rows * LANES // GROUP)
    for g in range(groups):
        wait_sent(gather_send.at[g], width)
        wait_sent(reduce_send.at[g], width)
    pltpu.make_async_copy(out_rows, out_ref, out_sem).wait()


def column_cuts(width):
    tiles, total = width // LANES, sum(part for _, part in PIECES)
    cuts, passed = [], 0
    for _, part in PIECES:
        first, end = (tiles * n // total * LANES for n in (passed, passed + part))
        cuts.append((first, end - first))
        passed += part
    return cuts


def layer_rows(
    queries, key_rows, value_rows, out_gate, decay_logit, head_gain, w_out,
    ffn_gain, routing, route_weight, residual_in, gate_cols, up_cols, down_rows,
):
    sp_count, tp_count = lax.axis_size("sp"), lax.axis_size("tp")
    rows, width = residual_in.shape
    tokens, key_lanes = queries.shape
    value_lanes = value_rows.shape[1]
    units = gate_cols.shape[1]
    z_count, groups = sp_count // 2, rows // GROUP
    group_rows = sp_count * tp_count * GROUP
    cuts = column_cuts(width)
    hbm = pl.BlockSpec(memory_space=pl.ANY)
    bf16, f32 = jnp.bfloat16, jnp.float32
    dma = pltpu.SemaphoreType.DMA
    operands = (
        queries, key_rows, value_rows, out_gate, decay_logit, head_gain.reshape(1, -1), w_out,
        ffn_gain.reshape(-1, LANES), routing.T, route_weight.T, residual_in,
        gate_cols, up_cols, down_rows,
    )

    def like(array):
        return pltpu.VMEM(array.shape, array.dtype)

    return pl.pallas_call(
        functools.partial(layer_kernel, sp_count, tp_count, cuts),
        out_shape=jax.ShapeDtypeStruct((rows, width), bf16),
        in_specs=[hbm] * len(operands),
        out_specs=hbm,
        scratch_shapes=[
            *(like(operands[i]) for i in (0, 1, 2, 3, 4, 5, 7, 8, 9, 10)),
            pltpu.VMEM((sp_count, DV, key_lanes), bf16),
            pltpu.VMEM((sp_count, 1, key_lanes), f32),
            pltpu.VMEM((tokens, value_lanes), f32),
            pltpu.VMEM((tokens, value_lanes), f32),
            pltpu.VMEM((tokens, value_lanes), bf16),
            pltpu.VMEM((tp_count - 1, rows, value_lanes), bf16),
            like(w_out),
            pltpu.VMEM((groups, z_count, 2, 2, 2, GROUP, width), bf16),
            pltpu.VMEM((z_count, 2, 2, 2, rows, LANES), bf16),
            like(gate_cols),
            like(up_cols),
            like(down_rows),
            pltpu.VMEM((groups, group_rows, units), bf16),
            pltpu.VMEM((groups, z_count, 2, 2, 2, GROUP, width), bf16),
            pltpu.VMEM((groups, z_count, 2, 2, GROUP, width), bf16),
            pltpu.VMEM((groups, z_count, 2, GROUP, width), bf16),
            pltpu.VMEM((groups, z_count, GROUP, width), bf16),
            pltpu.VMEM((groups, z_count - 1, 2, GROUP, width), bf16),
            pltpu.VMEM((groups, z_count - 1, GROUP, width), bf16),
            pltpu.VMEM((rows, width), bf16),
            dma((10,)),
            dma((4,)),
            dma,
            dma,
            dma,
            dma,
            dma,
            dma((tp_count - 1,)),
            dma,
            dma((4,)),
            dma((groups,)),
            dma((groups, len(cuts), 3)),
            dma((groups,)),
            dma((groups,)),
            dma((groups, len(cuts), 4)),
            dma,
        ],
        compiler_params=pltpu.CompilerParams(
            collective_id=1, has_side_effects=True, vmem_limit_bytes=62 << 20
        ),
        name="layer_rows",
    )(*operands)


def slot_ids(routes, capacity, experts):
    batch_size, rows_each, top_count = routes.shape
    flat_ids = routes.reshape(batch_size, rows_each * top_count)
    onehot = (flat_ids[:, :, None] == jnp.arange(experts, dtype=jnp.int32)[None, None, :]).astype(
        jnp.int32
    )
    earlier = jnp.cumsum(onehot, axis=1) - onehot
    rank_in = jnp.sum(earlier * onehot, axis=2)
    return (flat_ids * capacity + rank_in).reshape(batch_size, rows_each, top_count)


def dispatch_rows(slots, row_data, slot_total):
    chosen = jnp.any(slots[..., None] == jnp.arange(slot_total, dtype=jnp.int32), axis=2).astype(
        jnp.bfloat16
    )
    return jnp.einsum("brs,brd->bsd", chosen, row_data, preferred_element_type=jnp.float32).astype(
        jnp.bfloat16
    )


def on_device(
    residual_in,
    queries,
    key_rows,
    value_rows,
    out_gate,
    decay_logit,
    head_gain,
    w_out,
    ffn_gain,
    routing,
    route_weight,
    w_gate,
    w_up,
    w_down,
):
    tp_count = lax.axis_size("tp")
    experts = lax.axis_size("sp")
    quarter = residual_in.shape[0]
    top_count = routing.shape[1]
    model_width = residual_in.shape[1]
    capacity = 2 * routing.shape[0] * top_count // (tp_count * experts)
    slot_total = experts * capacity
    if (
        capacity >= quarter and experts <= LANES // 2 and experts % 4 == 0
        and tp_count == 4 and quarter % GROUP == 0
        and w_out.shape[0] >= (experts * tp_count - 1) * GROUP and model_width % (16 * LANES) == 0
        and quarter * LANES // GROUP <= model_width
    ):
        return layer_rows(
            queries, key_rows, value_rows, out_gate, decay_logit, head_gain, w_out,
            ffn_gain, routing, route_weight, residual_in, w_gate[0], w_up[0], w_down[0],
        )
    residual, extended = mix_rows(
        queries, key_rows, value_rows, out_gate, decay_logit, head_gain, w_out,
        ffn_gain, routing, route_weight, residual_in,
    )
    normed = extended[:, :model_width]
    gate_cols = w_gate[0]
    up_cols = w_up[0]
    down_rows = w_down[0]
    own_routes = lax.dynamic_slice_in_dim(routing, lax.axis_index("tp") * quarter, quarter, 0)
    own_slots = slot_ids(own_routes[None], capacity, experts)[0]
    outgoing = dispatch_rows(own_slots[None], normed[None], slot_total)[0]
    arrived = lax.all_to_all(
        outgoing.reshape(experts, capacity, model_width),
        "sp",
        split_axis=0,
        concat_axis=0,
        tiled=True,
    )
    portion = lax.all_gather(arrived[None], "tp", axis=0, tiled=True)
    flat_rows = portion.reshape(-1, model_width)
    gate_pre = jnp.dot(flat_rows, gate_cols, preferred_element_type=jnp.float32)
    up_pre = jnp.dot(flat_rows, up_cols, preferred_element_type=jnp.float32)
    hidden_rows = clamped_unit(gate_pre, up_pre).astype(jnp.bfloat16)
    hidden = hidden_rows.reshape(portion.shape[:-1] + (gate_cols.shape[1],))
    portion = hidden
    partial_out = jnp.dot(
        portion.reshape(-1, hidden.shape[-1]), down_rows, preferred_element_type=jnp.float32
    ).astype(jnp.bfloat16)
    partial_out = lax.optimization_barrier(partial_out)
    summed = lax.psum_scatter(
        partial_out.astype(jnp.float32)
        .reshape(portion.shape[:-1] + (model_width,))
        .astype(jnp.bfloat16),
        "tp",
        scatter_dimension=0,
        tiled=True,
    ).astype(jnp.float32)
    returned = lax.all_to_all(
        summed[0].astype(jnp.bfloat16), "sp", split_axis=0, concat_axis=0, tiled=True
    )
    picked = jnp.take(
        returned.reshape(slot_total, model_width), own_slots.reshape(-1), axis=0
    ).reshape(quarter, top_count, model_width)
    routed = jnp.sum(picked.astype(jnp.float32) * route_weight[:, :, None], axis=1)
    return (residual.astype(jnp.float32) + routed).astype(jnp.bfloat16)


def solution(mesh):
    placed = (
        P(("sp", "tp"), None),
        P("sp", "tp"),
        P("sp", "tp"),
        P("sp", "tp"),
        P("sp", "tp"),
        P("sp", "tp"),
        P(),
        P(),
        P(),
        P("sp", None),
        P(("sp", "tp"), None),
        P("sp", None, "tp"),
        P("sp", None, "tp"),
        P("sp", "tp", None),
    )
    return jax.shard_map(
        on_device, mesh=mesh, in_specs=placed, out_specs=P(("sp", "tp"), None), check_vma=False
    )
```
